32 devices in a mesh: sp: 8 (over z, x), tp: 4 (over y, core).
Axes of the slice: x: 2, y: 2, z: 4, core: 2. Of those that a mesh axis runs over, the one named last changes fastest.
Arguments:
- query_logits: bfloat16 [4096, 4096], P('sp', 'tp'), may hold values from -6 to 6
- forget_logits: bfloat16 [4096, 4096], P('sp', 'tp'), may hold values from -6 to 6
- value_inputs: bfloat16 [4096, 4096], P('sp', 'tp'), may hold values from -16 to 16
- output_gate_logits: bfloat16 [4096, 4096], P('sp', 'tp'), may hold values from -6 to 6
- forget_floor_gap: float32 [4096], replicated, may hold values from 2.4414063e-05 to 0.1
- surge_log_decay: float32 [32, 4096], P('tp', 'sp'), may hold values from -0.7 to 0
- head_norm_gain: float32 [128], replicated, may hold values from 0.1 to 1.9
- output_matrix: bfloat16 [4096, 4096], P('sp', 'tp'), may hold values from -1.25 to 1.25
- branch_norm_gain: float32 [4096], replicated, may hold values from 0.1 to 1.9
- residual: bfloat16 [4096, 4096], P('sp', 'tp'), may hold values from -6 to 6
Outputs:
- output: bfloat16 [4096, 4096], P('sp', 'tp')
The draws below stay inside these ranges and needn't reach their ends.
All inputs are finite; a program needn't handle non-finite values.
Results may differ from the reference program's by a relative error of at most 0.005.
Values may be sent and summed in bfloat16 or wider, within the bound.
A program may use at most 128 MiB of HBM per device.

```python
import math
import jax
import jax.numpy as jnp
from jax import lax

HEAD_DIM = 128
HEAD_TOTAL = 32
D = 4096
BLOCK_SPAN = 64
TOK_DEV = 512
TOKEN_TOTAL = 4096


surge_count = 3


def draw_forget_logits(key, part):
    leading_item, second = jax.random.split(key, 2)
    width = HEAD_TOTAL * HEAD_DIM
    offsets = jax.random.uniform(second, (TOKEN_TOTAL // TOK_DEV, 1, 1), jnp.float32, -1.5, 1.5)
    base = jnp.clip(jax.random.normal(leading_item, (TOKEN_TOTAL, width), jnp.float32), -4.0, 4.0)
    shifted = base.reshape(TOKEN_TOTAL // TOK_DEV, TOK_DEV, width) + offsets
    return shifted.reshape(TOKEN_TOTAL, width).astype(jnp.bfloat16)


def draw_forget_floor_gap(key, part):
    leading_item, second, third = jax.random.split(key, 3)
    share = 0.5
    quick = jax.random.uniform(leading_item, (HEAD_TOTAL, 1), jnp.float32) < share
    slow_gap = jax.random.uniform(second, (HEAD_TOTAL, HEAD_DIM), jnp.float32, 0.1, 0.6) / TOKEN_TOTAL
    quick_gap = jnp.exp(jax.random.uniform(third, (HEAD_TOTAL, HEAD_DIM), jnp.float32, math.log(0.03), math.log(0.1)))
    return jnp.where(quick, quick_gap, slow_gap).reshape(HEAD_TOTAL * HEAD_DIM)


def draw_surge_log_decay(key, part):
    leading_item, second = jax.random.split(key, 2)
    position_grid = jax.random.randint(leading_item, (HEAD_TOTAL, surge_count), 0, TOKEN_TOTAL)
    hits = jnp.any(jnp.arange(TOKEN_TOTAL)[None, :, None] == position_grid[:, None, :], axis=2)
    amounts = jnp.log(jax.random.uniform(second, (HEAD_TOTAL, TOKEN_TOTAL), jnp.float32, 0.5, 0.8))
    return jnp.where(hits, amounts, 0.0).astype(jnp.float32)


def draw_output_matrix(key, part):
    leading_item, second = jax.random.split(key, 2)
    width = HEAD_TOTAL * HEAD_DIM
    limit = 80.0 / math.sqrt(width)
    ramp = jnp.exp(math.log(3.0) * jnp.arange(D).astype(jnp.float32) / D)
    base = jnp.clip(jax.random.normal(leading_item, (width, D), jnp.float32), -4.0, 4.0)
    column_scale = ramp * jnp.exp(jax.random.uniform(second, (D,), jnp.float32, 0.0, math.log(4.0)))
    values = jnp.clip(base * column_scale / math.sqrt(width), -limit, limit)
    return values.astype(jnp.bfloat16)


def shard_levels(key, extent, cuts, least, top_value):
    def one(dim, parts):
        draws = jax.random.uniform(jax.random.fold_in(jax.random.fold_in(key, 6), dim), (parts,), jnp.float32, least / len(cuts), top_value / len(cuts))
        return jnp.repeat(jnp.exp(draws), extent[dim] // parts).reshape((-1,) + (1,) * (len(extent) - dim - 1))

    loudness = one(*cuts[0])
    for cut in cuts[1:]:
        loudness = loudness * one(*cut)
    return loudness


def noise(own_key, dims, deviation, reach, cuts=(), kind=jnp.bfloat16):
    values = jax.random.normal(own_key, dims, jnp.float32) * deviation
    if len(cuts) > 0:
        values = shard_levels(own_key, dims, cuts, -0.22, 0.18) * values
    return jnp.clip(values, min=-reach, max=reach).astype(kind)


def setup_inputs(seed: int = 0) -> dict:
    arg_keys = jax.random.split(jax.random.key(seed), 11)
    return {
        "query_logits": noise(arg_keys[0], (TOKEN_TOTAL, HEAD_TOTAL * HEAD_DIM), 1.0, 6.0, ((0, 8), (1, 4))),
        "forget_logits": draw_forget_logits(jax.random.fold_in(arg_keys[10], 71), 0),
        "value_inputs": noise(arg_keys[2], (TOKEN_TOTAL, HEAD_TOTAL * HEAD_DIM), 4.0, 16.0, ((0, 8), (1, 4))),
        "output_gate_logits": noise(arg_keys[3], (TOKEN_TOTAL, HEAD_TOTAL * HEAD_DIM), 1.0, 6.0, ((0, 8), (1, 4))),
        "forget_floor_gap": draw_forget_floor_gap(jax.random.fold_in(arg_keys[10], 71), 0),
        "surge_log_decay": draw_surge_log_decay(jax.random.fold_in(arg_keys[10], 71), 0),
        "head_norm_gain": jnp.clip(1.0 + 0.18 * jax.random.normal(arg_keys[6], (HEAD_DIM,), jnp.float32), 0.1, 1.9),
        "output_matrix": draw_output_matrix(jax.random.fold_in(arg_keys[10], 71), 0),
        "branch_norm_gain": jnp.clip(1.0 + 0.18 * jax.random.normal(arg_keys[8], (D,), jnp.float32), 0.1, 1.9),
        "residual": noise(arg_keys[9], (TOKEN_TOTAL, D), 1.0, 6.0, ((0, 8), (1, 4))),
    }


epsilon = 1e-06

def block_update(state, queries, keys_in, values_in, running):
    length = running.shape[1]
    middle = length // 2
    anchor = running[:, middle - 1:middle, :]
    ending = running[:, -1:, :]
    causal = jnp.tril(jnp.ones((length, length), dtype=bool))
    highest = lax.Precision.HIGHEST
    inter = jnp.einsum('htd,hde->hte', queries * jnp.exp(running), state, precision=highest)
    scores = jnp.einsum('htd,hsd->hts', queries * jnp.exp(running - anchor), keys_in * jnp.exp(anchor - running), precision=highest)
    intra = jnp.einsum('hts,hse->hte', jnp.where(causal[None], scores, 0.0), values_in, precision=highest)
    new_state = state * jnp.exp(ending[:, 0, :])[:, :, None] + jnp.einsum('hsd,hse->hde', keys_in * jnp.exp(ending - running), values_in, precision=highest)
    return (new_state, inter + intra)

def head_gates(query_logits, forget_logits, value_inputs, gap):
    row_count = query_logits.shape[0]
    head_count = query_logits.shape[1] // HEAD_DIM

    def shaped(array):
        return array.astype(jnp.float32).reshape(row_count, head_count, HEAD_DIM)
    queries = jax.nn.silu(shaped(query_logits)) * HEAD_DIM ** (-0.5)
    keys_in = gap.reshape(head_count, HEAD_DIM) * jax.nn.sigmoid(-shaped(forget_logits))
    values_in = shaped(value_inputs)
    decay_factors = jnp.log1p(-keys_in)
    return (queries, keys_in, values_in, decay_factors)

def gated_norm(heads_out, output_gate_logits, head_norm_gain):
    mean_sq = lax.optimization_barrier(jnp.mean(heads_out * heads_out, axis=-1, keepdims=True))
    gates = jax.nn.silu(output_gate_logits.astype(jnp.float32).reshape(heads_out.shape))
    normed = heads_out * lax.rsqrt(mean_sq + epsilon) * head_norm_gain * gates
    return normed.reshape(heads_out.shape[0], -1).astype(jnp.bfloat16)

def reference(query_logits, forget_logits, value_inputs, output_gate_logits, forget_floor_gap, surge_log_decay, head_norm_gain, output_matrix, branch_norm_gain, residual):
    number_of_blocks = TOKEN_TOTAL // BLOCK_SPAN

    def split_into_blocks(array):
        return array.reshape(number_of_blocks, BLOCK_SPAN, array.shape[1])
    surge_values = jnp.transpose(surge_log_decay).reshape(number_of_blocks, BLOCK_SPAN, HEAD_TOTAL)

    def step_forward(state, input_tuple):
        query_tile_block, forget_gate_block, value_rows_block, output_gate_block, surge_block, residual_block = input_tuple
        queries, keys_in, values_in, decay_factors = head_gates(query_tile_block, forget_gate_block, value_rows_block, forget_floor_gap)
        decay_factors = decay_factors + surge_block[:, :, None]
        running = jnp.cumsum(jnp.transpose(decay_factors, (1, 0, 2)), axis=1)
        new_state, heads_out = block_update(state, jnp.transpose(queries, (1, 0, 2)), jnp.transpose(keys_in, (1, 0, 2)), jnp.transpose(values_in, (1, 0, 2)), running)
        mixed_rows = gated_norm(jnp.transpose(heads_out, (1, 0, 2)), output_gate_block, head_norm_gain)
        projected = lax.optimization_barrier(jnp.dot(mixed_rows, output_matrix, preferred_element_type=jnp.float32).astype(jnp.bfloat16))
        branch = projected.astype(jnp.float32)
        scale = lax.rsqrt(lax.optimization_barrier(jnp.mean(branch * branch, axis=-1, keepdims=True)) + epsilon)
        result = (residual_block.astype(jnp.float32) + branch * scale * branch_norm_gain).astype(jnp.bfloat16)
        return (new_state, result)
    starting_state = jnp.zeros((HEAD_TOTAL, HEAD_DIM, HEAD_DIM), jnp.float32)
    unused_slot, output_list = lax.scan(step_forward, starting_state, (split_into_blocks(query_logits), split_into_blocks(forget_logits), split_into_blocks(value_inputs), split_into_blocks(output_gate_logits), surge_values, split_into_blocks(residual)))
    return output_list.reshape(TOKEN_TOTAL, D)
```

```python
import functools

import jax
import jax.numpy as jnp
from jax import lax
from jax.experimental import pallas as pl
from jax.experimental.pallas import tpu as pltpu
from jax.sharding import Mesh
from jax.sharding import PartitionSpec as P

HEAD_DIM = 128
SPAN = 128
TAIL = 16
EPSILON = 1e-06
NT = (((1,), (1,)), ((), ()))
TN = (((0,), (0,)), ((), ()))
NN = (((1,), (0,)), ((), ()))
MESH_ID = pl.DeviceIdType.MESH


def dot(a, b, dims=NN):
    return lax.dot_general(a, b, dims, preferred_element_type=jnp.float32)


def lower_triangle():
    rows = lax.broadcasted_iota(jnp.int32, (SPAN, SPAN), 0)
    columns = lax.broadcasted_iota(jnp.int32, (SPAN, SPAN), 1)
    return rows >= columns


def diagonal():
    rows = lax.broadcasted_iota(jnp.int32, (SPAN, SPAN), 0)
    columns = lax.broadcasted_iota(jnp.int32, (SPAN, SPAN), 1)
    return rows == columns


def silu(logits):
    return logits / (1.0 + jnp.exp(-logits))


def decays(logits, gap, surge, causal):
    keys = gap / (1.0 + jnp.exp(logits.astype(jnp.float32)))
    series = keys * (1.0 / 7.0) + (1.0 / 6.0)
    for order in (5, 4, 3, 2):
        series = series * keys + (1.0 / order)
    logs = -(series * keys + 1.0) * keys
    high = logs.astype(jnp.bfloat16)
    low = (logs - high.astype(jnp.float32)).astype(jnp.bfloat16)
    ones = causal.astype(jnp.bfloat16)
    surged = jnp.sum(jnp.where(causal, surge, 0.0), axis=1, keepdims=True)
    return keys, dot(ones, high) + dot(ones, low) + surged


def layer_kernel(
    sizes,
    query_in,
    forget_in,
    value_in,
    gate_in,
    gap_ref,
    surge_ref,
    gain_ref,
    weight_in,
    branch_gain_ref,
    residual_in,
    out_hbm,
    whole_weight,
    query_ref,
    forget_ref,
    value_ref,
    gate_ref,
    residual_ref,
    running_ref,
    keys_ref,
    base_ref,
    starts_ref,
    state_out,
    gathered,
    prefix,
    carried,
    local_ref,
    reach_ref,
    gated_ref,
    mixed_ref,
    partial_out,
    partial_in,
    here_ref,
    projected_ref,
    squares_ref,
    out_ref,
    load_sems,
    gather_send,
    gather_recv,
    return_send,
    return_recv,
    swap_sems,
    tp_sems,
    line_sems,
    side_sems,
    partial_sems,
    square_send,
    square_recv,
    store_sems,
):
    hi_size, inner_size, tp_size, per, tile, weight_tile = sizes
    places = 2 * hi_size * inner_size
    rows, width = query_in.shape
    depth, columns = weight_in.shape
    heads = width // HEAD_DIM
    spans = rows // SPAN
    groups = heads // per
    half_width = heads * tp_size // 2 * HEAD_DIM
    stride = places // heads
    tiles = columns // tile
    pieces = columns // weight_tile
    ratio = tile // weight_tile
    hi, lo, inner, tp = (lax.axis_index(a) for a in ("hi", "lo", "inner", "tp"))
    place = (hi * 2 + lo) * inner_size + inner
    strides = []
    by = tp_size // 2
    while by >= 1:
        strides.append(by)
        by //= 2

    def at(position):
        return {
            "hi": position // (2 * inner_size),
            "lo": (position // inner_size) % 2,
            "inner": position % inner_size,
        }

    def flipped(index, by):
        return index + by - 2 * by * ((index // by) % 2)

    def remote(source, target, send, recv, device):
        return pltpu.make_async_remote_copy(
            src_ref=source,
            dst_ref=target,
            send_sem=send,
            recv_sem=recv,
            device_id=device,
            device_id_type=MESH_ID,
        )

    def span_rows(span):
        return pl.ds(span * SPAN, SPAN)

    def lanes_of(head):
        return pl.ds(pl.multiple_of(head * HEAD_DIM, HEAD_DIM), HEAD_DIM)

    def slot_rows(block_hi, block_inner):
        return pl.ds(pl.multiple_of((block_hi * inner_size + block_inner) * depth, depth), depth)

    loads = [
        pltpu.make_async_copy(source, target, load_sems.at[number])
        for number, (source, target) in enumerate(
            (
                (forget_in, forget_ref),
                (value_in, value_ref),
                (weight_in, whole_weight.at[slot_rows(hi, inner)]),
                (query_in, query_ref),
                (gate_in, gate_ref),
                (residual_in, residual_ref),
            )
        )
    ]
    for load in loads:
        load.start()

    barrier = pltpu.get_barrier_semaphore()

    def greet(position, carry):
        @pl.when(position != place)
        def _():
            pl.semaphore_signal(barrier, inc=1, device_id=at(position), device_id_type=MESH_ID)

        return carry

    lax.fori_loop(0, places, greet, 0)
    for step in range(1, tp_size):
        pl.semaphore_signal(
            barrier, inc=1, device_id={"tp": (tp + step) % tp_size}, device_id_type=MESH_ID
        )
    pl.semaphore_wait(barrier, places - 1 + tp_size - 1)

    def weight_block(block_hi, block_inner, piece):
        return whole_weight.at[
            slot_rows(block_hi, block_inner), pl.ds(piece * weight_tile, weight_tile)
        ]

    def step_of(way):
        return 1 if way == 0 else -1

    def line_copy(way, hop, piece):
        block = weight_block(hi - step_of(way) * (hop - 1), inner, piece)
        return remote(
            block,
            block,
            line_sems.at[0, way, hop - 1, piece],
            line_sems.at[1, way, hop - 1, piece],
            {"hi": hi + step_of(way)},
        )

    def sends(way, hop):
        origin = hi - step_of(way) * (hop - 1)
        target = hi + step_of(way)
        return (origin >= 0) & (origin < hi_size) & (target >= 0) & (target < hi_size)

    def receives(way, hop):
        origin = hi - step_of(way) * hop
        return (origin >= 0) & (origin < hi_size)

    def side_copy(reach, block_hi, piece):
        block = weight_block(block_hi, inner, piece)
        return remote(
            block,
            block,
            side_sems.at[0, reach - 1, block_hi, piece],
            side_sems.at[1, reach - 1, block_hi, piece],
            {"inner": (inner + reach) % inner_size},
        )

    def start_line(piece):
        for way in (0, 1):

            @pl.when(sends(way, 1))
            def _():
                line_copy(way, 1, piece).start()

    def start_side(piece):
        for reach in range(1, inner_size):
            side_copy(reach, hi, piece).start()

    def pass_weight(piece):
        for hop in range(1, hi_size):
            for way in (0, 1):

                @pl.when(receives(way, hop))
                def _():
                    line_copy(way, hop, piece).wait_recv()
                    for reach in range(1, inner_size):
                        side_copy(reach, hi - step_of(way) * hop, piece).start()

                if hop + 1 < hi_size:

                    @pl.when(sends(way, hop + 1))
                    def _():
                        line_copy(way, hop + 1, piece).start()

    def need_weight(piece):
        for reach in range(1, inner_size):
            for block_hi in range(hi_size):
                side_copy(reach, block_hi, piece).wait_recv()

    def state_copy(head):
        return remote(
            state_out.at[head],
            gathered.at[place],
            gather_send.at[head],
            gather_recv.at[place],
            at(head * stride),
        )

    def state_arrival(position):
        return remote(
            state_out.at[0],
            gathered.at[position],
            gather_send.at[0],
            gather_recv.at[position],
            at(position),
        )

    def prefix_copy(position, head):
        return remote(
            prefix.at[position],
            carried.at[head],
            return_send.at[position],
            return_recv.at[head],
            at(position),
        )

    def state_body(head, carry):
        causal = lower_triangle()
        gap = gap_ref[pl.ds(tp * heads + head, 1), :]
        lanes = lanes_of(head)
        this_head = lax.broadcasted_iota(jnp.int32, (heads, SPAN), 0) == head
        state = jnp.zeros((HEAD_DIM, HEAD_DIM), jnp.float32)
        base = jnp.zeros((1, HEAD_DIM), jnp.float32)
        for span in range(spans):
            part = span_rows(span)
            surge = jnp.sum(jnp.where(this_head, surge_ref[:, part], 0.0), axis=0, keepdims=True)
            keys, running = decays(forget_ref[part, lanes], gap, surge, causal)
            keys_ref[part, lanes] = keys
            running_ref[part, lanes] = running
            base_ref[head, span : span + 1, :] = base
            if span > 0:
                starts_ref[head, span - 1] = state.astype(jnp.bfloat16)
            ending = running[SPAN - 1 : SPAN, :]
            kept = (keys * jnp.exp(ending - running)).astype(jnp.bfloat16)
            state = state * jnp.exp(ending) + dot(value_ref[part, lanes], kept, TN)
            base = base + ending
        decay = jnp.exp(base)
        high = decay.astype(jnp.bfloat16).astype(jnp.float32)
        first = lax.broadcasted_iota(jnp.int32, (TAIL, HEAD_DIM), 0) == 0
        item = state.astype(jnp.bfloat16)
        tail = jnp.where(first, high, decay - high).astype(jnp.bfloat16)
        state_out[head, 0:HEAD_DIM, :] = item
        state_out[head, HEAD_DIM:, :] = tail
        owner = head * stride

        @pl.when(owner == place)
        def _():
            gathered[place, 0:HEAD_DIM, :] = item
            gathered[place, HEAD_DIM:, :] = tail

        @pl.when((owner != place) & (place < places - 1))
        def _():
            state_copy(head).start()

        return carry

    def scan_states():
        @pl.when(place % stride == 0)
        def _():
            mine = place // stride

            def body(position, carry):
                @pl.when(position != place)
                def _():
                    state_arrival(position).wait_recv()

                tail = gathered[position, HEAD_DIM:, :].astype(jnp.float32)
                decay = tail[0:1, :] + tail[1:2, :]
                carry = carry * decay + gathered[position, 0:HEAD_DIM, :].astype(jnp.float32)
                later = position + 1
                prefix[later] = carry.astype(jnp.bfloat16)

                @pl.when(later == place)
                def _():
                    carried[mine] = carry.astype(jnp.bfloat16)

                @pl.when(later != place)
                def _():
                    prefix_copy(later, mine).start()

                return carry

            lax.fori_loop(0, places - 1, body, jnp.zeros((HEAD_DIM, HEAD_DIM), jnp.float32))

    def take_states():
        @pl.when(place == 0)
        def _():
            carried[...] = jnp.zeros_like(carried)

        @pl.when(place > 0)
        def _():
            def body(head, carry):
                @pl.when(head * stride != place)
                def _():
                    prefix_copy(0, head).wait_recv()

                return carry

            lax.fori_loop(0, heads, body, 0)

    gain = gain_ref[...]

    def local_body(head, carry):
        causal = lower_triangle()
        lanes = lanes_of(head)
        middle = SPAN // 2
        for span in range(spans):
            part = span_rows(span)
            running = running_ref[part, lanes]
            anchor = running[middle - 1 : middle, :]
            queries = silu(query_ref[part, lanes].astype(jnp.float32)) * (HEAD_DIM**-0.5)
            reach = queries * jnp.exp(running - anchor)
            back = keys_ref[part, lanes] * jnp.exp(anchor - running)
            scores = dot(reach.astype(jnp.bfloat16), back.astype(jnp.bfloat16), NT)
            scores = jnp.where(causal, scores, 0.0).astype(jnp.bfloat16)
            out = dot(scores, value_ref[part, lanes])
            if span > 0:
                out = out + dot(
                    (reach * jnp.exp(anchor)).astype(jnp.bfloat16), starts_ref[head, span - 1], NT
                )
            local_ref[part, lanes] = out
            base = base_ref[head, span : span + 1, :]
            reach_ref[part, lanes] = (reach * jnp.exp(anchor + base)).astype(jnp.bfloat16)
            gated_ref[part, lanes] = gain * silu(gate_ref[part, lanes].astype(jnp.float32))
        return carry

    def keeps(index, group):
        return (index * groups + group) % 2 == lo

    def group_lanes(index, group, which):
        start = which * half_width + (index * groups + group) // 2 * per * HEAD_DIM
        return pl.ds(pl.multiple_of(start, HEAD_DIM), per * HEAD_DIM)

    def swap_copy(group, span):
        start = 2 * half_width + group * per * HEAD_DIM
        return remote(
            mixed_ref.at[span_rows(span), pl.ds(start, per * HEAD_DIM)],
            mixed_ref.at[span_rows(span), group_lanes(tp, group, 1)],
            swap_sems.at[0, group, span],
            swap_sems.at[1, group, span],
            {"lo": 1 - lo},
        )

    def origin_of(index, mask):
        for bit, by in enumerate(strides):
            if (mask >> bit) & 1:
                index = flipped(index, by)
        return index

    def tp_copy(stage, which, mask, group, span):
        block = mixed_ref.at[span_rows(span), group_lanes(origin_of(tp, mask), group, which)]
        return remote(
            block,
            block,
            tp_sems.at[0, stage, which, mask, group, span],
            tp_sems.at[1, stage, which, mask, group, span],
            {"tp": flipped(tp, strides[stage])},
        )

    def mix(span):
        part = span_rows(span)
        for head in range(heads):
            lanes = lanes_of(head)
            out = local_ref[part, lanes] + dot(reach_ref[part, lanes], carried[head], NT)
            mean_sq = jnp.mean(out * out, axis=1, keepdims=True)
            mixed = out * lax.rsqrt(mean_sq + EPSILON) * gated_ref[part, lanes]
            group = head // per
            kept_start = (tp * groups + group) // 2 * per * HEAD_DIM + head % per * HEAD_DIM
            away_start = 2 * half_width + head * HEAD_DIM
            start = jnp.where(keeps(tp, group), kept_start, away_start)
            mixed_ref[part, pl.ds(pl.multiple_of(start, HEAD_DIM), HEAD_DIM)] = mixed.astype(
                jnp.bfloat16
            )

    def send_mixed(span):
        for group in range(groups):

            @pl.when(keeps(tp, group))
            def _():
                for stage in range(len(strides)):
                    tp_copy(stage, 0, 0, group, span).start()

            @pl.when(jnp.logical_not(keeps(tp, group)))
            def _():
                swap_copy(group, span).start()

    def take_swap(span):
        for group in range(groups):

            @pl.when(keeps(tp, group))
            def _():
                swap_copy(group, span).wait_recv()
                for stage in range(len(strides)):
                    tp_copy(stage, 1, 0, group, span).start()

    def take_stage(stage, which, span):
        peer = flipped(tp, strides[stage])
        for mask in range(1 << stage):
            for group in range(groups):

                @pl.when(keeps(origin_of(peer, mask), group))
                def _():
                    tp_copy(stage, which, mask, group, span).wait_recv()
                    for later in range(stage + 1, len(strides)):
                        tp_copy(later, which, mask | (1 << stage), group, span).start()

    def partial_copy(span, number):
        return remote(
            partial_out.at[span, number],
            partial_in.at[span, number],
            partial_sems.at[0, span, number],
            partial_sems.at[1, span, number],
            {"lo": 1 - lo},
        )

    def multiply(span, number):
        part = span_rows(span)
        both = jnp.concatenate(
            [mixed_ref[part, half_width : 2 * half_width], mixed_ref[part, 0:half_width]], axis=0
        )
        product = dot(both, whole_weight[:, number * tile : (number + 1) * tile])
        partial_out[span, number] = product[0:SPAN].astype(jnp.bfloat16)
        partial_copy(span, number).start()
        here_ref[span, number] = product[SPAN:]

    def square_copy(step, span):
        return remote(
            squares_ref.at[tp, span],
            squares_ref.at[tp, span],
            square_send.at[step - 1, span],
            square_recv.at[step - 1, span],
            {"tp": (tp + step) % tp_size},
        )

    def combine(span):
        part = span_rows(span)
        squares = jnp.zeros((SPAN, HEAD_DIM), jnp.float32)
        for number in range(tiles):
            partial_copy(span, number).wait_recv()
            total = here_ref[span, number] + partial_in[span, number].astype(jnp.float32)
            rounded = total.astype(jnp.bfloat16)
            projected_ref[part, number * tile : (number + 1) * tile] = rounded
            branch = rounded.astype(jnp.float32)
            branch = branch * branch
            for start in range(0, tile, HEAD_DIM):
                squares = squares + branch[:, start : start + HEAD_DIM]
        column = jnp.sum(squares, axis=1, keepdims=True)
        row = jnp.sum(jnp.where(diagonal(), column, 0.0), axis=0, keepdims=True)
        squares_ref[tp, span] = jnp.broadcast_to(row, (8, HEAD_DIM))
        for step in range(1, tp_size):
            square_copy(step, span).start()

    def store_copy(span):
        return pltpu.make_async_copy(
            out_ref.at[span_rows(span)], out_hbm.at[span_rows(span)], store_sems.at[span]
        )

    def finish(span):
        part = span_rows(span)
        for step in range(1, tp_size):
            square_copy(step, span).wait_recv()
        total = squares_ref[0, span, 0:1, :]
        for index in range(1, tp_size):
            total = total + squares_ref[index, span, 0:1, :]
        row = lax.rsqrt(total * (1.0 / (columns * tp_size)) + EPSILON)
        scale = jnp.sum(jnp.where(diagonal(), row, 0.0), axis=1, keepdims=True)
        for number in range(columns // HEAD_DIM):
            lanes = pl.ds(number * HEAD_DIM, HEAD_DIM)
            gain_row = branch_gain_ref[pl.ds(tp * (columns // HEAD_DIM) + number, 1), :]
            branch = projected_ref[part, lanes].astype(jnp.float32) * scale * gain_row
            out_ref[part, lanes] = (residual_ref[part, lanes].astype(jnp.float32) + branch).astype(
                jnp.bfloat16
            )
        store_copy(span).start()

    started_line, started_side, passed, needed = 0, 0, 0, 0

    def lines(until):
        nonlocal started_line
        while started_line < min(until, pieces):
            start_line(started_line)
            started_line += 1

    def sides(until):
        nonlocal started_side
        while started_side < min(until, pieces):
            start_side(started_side)
            started_side += 1

    def passes(until):
        nonlocal passed
        while passed < min(until, pieces):
            pass_weight(passed)
            passed += 1

    def needs(until):
        nonlocal needed
        while needed < min(until, pieces):
            need_weight(needed)
            needed += 1

    loads[2].wait()
    lines(1)
    sides(1)
    loads[0].wait()
    loads[1].wait()
    lax.fori_loop(0, heads, state_body, 0)
    lines(2)
    sides(3)
    loads[3].wait()
    loads[4].wait()
    first_heads = heads // 2
    lax.fori_loop(0, first_heads, local_body, 0)
    passes(1)
    scan_states()
    lines(4)
    sides(5)
    passes(2)
    lax.fori_loop(first_heads, heads, local_body, 0)
    passes(3)
    take_states()
    mix(0)
    send_mixed(0)
    mix(1)
    send_mixed(1)
    lines(6)
    sides(8)
    take_swap(0)
    mix(2)
    send_mixed(2)
    take_swap(1)
    mix(3)
    send_mixed(3)
    for span in range(4, spans):
        mix(span)
        send_mixed(span)
    lines(pieces)
    sides(pieces)
    passes(4)
    take_stage(0, 0, 0)
    for span in range(2, spans):
        take_swap(span)
        take_stage(0, 0, span - 1)
        take_stage(0, 1, span - 2)
    passes(6)
    take_stage(0, 0, spans - 1)
    loads[5].wait()
    for span in range(spans):
        if span >= spans - 2:
            take_stage(0, 1, span)
        for stage in range(1, len(strides)):
            for which in (0, 1):
                take_stage(stage, which, span)
        for number in range(tiles):
            passes((number + 1) * ratio)
            needs((number + 1) * ratio)
            multiply(span, number)
        if span >= 1:
            combine(span - 1)
        if span >= 2:
            finish(span - 2)
    combine(spans - 1)
    if spans >= 2:
        finish(spans - 2)
    finish(spans - 1)

    for piece in range(pieces):
        for way in (0, 1):
            for hop in range(1, hi_size):

                @pl.when(sends(way, hop))
                def _():
                    line_copy(way, hop, piece).wait_send()

        for reach in range(1, inner_size):
            for block_hi in range(hi_size):
                side_copy(reach, block_hi, piece).wait_send()

    def sent_state(head, carry):
        @pl.when((head * stride != place) & (place < places - 1))
        def _():
            state_copy(head).wait_send()

        return carry

    lax.fori_loop(0, heads, sent_state, 0)

    @pl.when(place % stride == 0)
    def _():
        def sent_prefix(position, carry):
            @pl.when(position != place)
            def _():
                prefix_copy(position, 0).wait_send()

            return carry

        lax.fori_loop(1, places, sent_prefix, 0)

    for span in range(spans):
        for group in range(groups):

            @pl.when(jnp.logical_not(keeps(tp, group)))
            def _():
                swap_copy(group, span).wait_send()

            for stage in range(len(strides)):
                for which in (0, 1):
                    for mask in range(1 << stage):

                        @pl.when(keeps(origin_of(tp, mask), group))
                        def _():
                            tp_copy(stage, which, mask, group, span).wait_send()

        for number in range(tiles):
            partial_copy(span, number).wait_send()
        for step in range(1, tp_size):
            square_copy(step, span).wait_send()
        store_copy(span).wait()


def layer(sizes, arrays):
    hi_size, inner_size, tp_size, per, tile, weight_tile = sizes
    rows, width = arrays[0].shape
    depth, columns = arrays[7].shape
    heads = width // HEAD_DIM
    groups = heads // per
    spans = rows // SPAN
    places = 2 * hi_size * inner_size
    stages = tp_size.bit_length() - 1
    half_width = heads * tp_size // 2 * HEAD_DIM
    tiles = columns // tile
    pieces = columns // weight_tile
    vmem = pl.BlockSpec(memory_space=pltpu.VMEM)
    anywhere = pl.BlockSpec(memory_space=pl.ANY)
    item = (HEAD_DIM + TAIL, HEAD_DIM)
    square = (HEAD_DIM, HEAD_DIM)
    bf16, f32 = jnp.bfloat16, jnp.float32
    dma = pltpu.SemaphoreType.DMA
    return pl.pallas_call(
        functools.partial(layer_kernel, sizes),
        in_specs=[anywhere] * 4 + [vmem] * 3 + [anywhere, vmem, anywhere],
        out_specs=anywhere,
        out_shape=jax.ShapeDtypeStruct((rows, columns), bf16),
        scratch_shapes=[
            pltpu.VMEM((hi_size * inner_size * depth, columns), bf16),
            pltpu.VMEM((rows, width), bf16),
            pltpu.VMEM((rows, width), bf16),
            pltpu.VMEM((rows, width), bf16),
            pltpu.VMEM((rows, width), bf16),
            pltpu.VMEM((rows, columns), bf16),
            pltpu.VMEM((rows, width), f32),
            pltpu.VMEM((rows, width), f32),
            pltpu.VMEM((heads, max(8, spans), HEAD_DIM), f32),
            pltpu.VMEM((heads, max(1, spans - 1)) + square, bf16),
            pltpu.VMEM((heads,) + item, bf16),
            pltpu.VMEM((places,) + item, bf16),
            pltpu.VMEM((places,) + square, bf16),
            pltpu.VMEM((heads,) + square, bf16),
            pltpu.VMEM((rows, width), f32),
            pltpu.VMEM((rows, width), bf16),
            pltpu.VMEM((rows, width), f32),
            pltpu.VMEM((rows, 2 * half_width + width), bf16),
            pltpu.VMEM((spans, tiles, SPAN, tile), bf16),
            pltpu.VMEM((spans, tiles, SPAN, tile), bf16),
            pltpu.VMEM((spans, tiles, SPAN, tile), f32),
            pltpu.VMEM((rows, columns), bf16),
            pltpu.VMEM((tp_size, spans, 8, HEAD_DIM), f32),
            pltpu.VMEM((rows, columns), bf16),
            dma((6,)),
            dma((heads,)),
            dma((places,)),
            dma((places,)),
            dma((heads,)),
            dma((2, groups, spans)),
            dma((2, stages, 2, tp_size // 2, groups, spans)),
            dma((2, 2, max(1, hi_size - 1), pieces)),
            dma((2, inner_size - 1, hi_size, pieces)),
            dma((2, spans, tiles)),
            dma((tp_size - 1, spans)),
            dma((tp_size - 1, spans)),
            dma((spans,)),
        ],
        name="layer",
        compiler_params=pltpu.CompilerParams(
            collective_id=0, has_side_effects=True, vmem_limit_bytes=60000 * 1024
        ),
        cost_estimate=pl.CostEstimate(
            flops=rows * width * 10000, bytes_accessed=14 * rows * width, transcendentals=0
        ),
    )(*arrays)


def per_device(hi_size, inner_size, tp_size, *arrays):
    query, forget, value, gate, gap, surge, head_gain, matrix, branch_gain, residual = arrays
    per = inner_size * matrix.shape[0] // HEAD_DIM
    return layer(
        (hi_size, inner_size, tp_size, per, 256, 128),
        (
            query,
            forget,
            value,
            gate,
            gap.reshape(-1, HEAD_DIM),
            surge,
            head_gain.reshape(1, HEAD_DIM),
            matrix,
            branch_gain.reshape(-1, HEAD_DIM),
            residual,
        ),
    )


def solution(mesh):
    sp_size, tp_size = mesh.shape["sp"], mesh.shape["tp"]
    sp = ("hi", "lo", "inner")
    placed = (
        P(sp, "tp"),
        P(sp, "tp"),
        P(sp, "tp"),
        P(sp, "tp"),
        P(),
        P("tp", sp),
        P(),
        P(sp, "tp"),
        P(),
        P(sp, "tp"),
    )

    def whole(*arrays):
        inner = max(2, HEAD_DIM * sp_size // arrays[7].shape[0])
        hi = sp_size // (2 * inner)
        devices = mesh.devices.reshape(hi, 2, inner, tp_size)
        paired = Mesh(devices, ("hi", "lo", "inner", "tp"))
        return jax.shard_map(
            functools.partial(per_device, hi, inner, tp_size),
            mesh=paired,
            in_specs=placed,
            out_specs=P(sp, "tp"),
            check_vma=False,
        )(*arrays)

    return whole
```

```python
import functools

import jax
import jax.numpy as jnp
from jax import lax
from jax.experimental import pallas as pl
from jax.experimental.pallas import tpu as pltpu
from jax.sharding import Mesh
from jax.sharding import PartitionSpec as P

HEAD_DIM = 128
SPAN = 128
TAIL = 16
EPSILON = 1e-06
NT = (((1,), (1,)), ((), ()))
TN = (((0,), (0,)), ((), ()))
NN = (((1,), (0,)), ((), ()))
MESH_ID = pl.DeviceIdType.MESH


def dot(a, b, dims=NN):
    return lax.dot_general(a, b, dims, preferred_element_type=jnp.float32)


def lower_triangle():
    rows = lax.broadcasted_iota(jnp.int32, (SPAN, SPAN), 0)
    columns = lax.broadcasted_iota(jnp.int32, (SPAN, SPAN), 1)
    return rows >= columns


def diagonal():
    rows = lax.broadcasted_iota(jnp.int32, (SPAN, SPAN), 0)
    columns = lax.broadcasted_iota(jnp.int32, (SPAN, SPAN), 1)
    return rows == columns


def silu(logits):
    return logits / (1.0 + jnp.exp(-logits))


def decays(logits, gap, surge, causal):
    keys = gap / (1.0 + jnp.exp(logits.astype(jnp.float32)))
    series = keys * (1.0 / 7.0) + (1.0 / 6.0)
    for order in (5, 4, 3, 2):
        series = series * keys + (1.0 / order)
    logs = -(series * keys + 1.0) * keys
    high = logs.astype(jnp.bfloat16)
    low = (logs - high.astype(jnp.float32)).astype(jnp.bfloat16)
    ones = causal.astype(jnp.bfloat16)
    surged = jnp.sum(jnp.where(causal, surge, 0.0), axis=1, keepdims=True)
    return keys, dot(ones, high) + dot(ones, low) + surged


def layer_kernel(
    sizes,
    query_in,
    forget_in,
    value_in,
    gate_in,
    gap_ref,
    surge_ref,
    gain_ref,
    weight_in,
    projected_hbm,
    scale_hbm,
    whole_weight,
    query_ref,
    forget_ref,
    value_ref,
    gate_ref,
    running_ref,
    keys_ref,
    base_ref,
    starts_ref,
    state_out,
    gathered,
    chain_in,
    chain_out,
    deliver_out,
    carried,
    local_ref,
    reach_ref,
    gated_ref,
    mixed_ref,
    partial_out,
    partial_in,
    total_ref,
    projected_ref,
    sums_ref,
    squares_ref,
    scale_ref,
    load_sems,
    gather_send,
    gather_recv,
    chain_sems,
    deliver_send,
    deliver_recv,
    swap_sems,
    tp_sems,
    line_sems,
    side_sems,
    partial_sems,
    square_send,
    square_recv,
    store_sems,
):
    hi_size, inner_size, tp_size, per, tile, weight_tile = sizes
    rows, width = query_in.shape
    depth, columns = weight_in.shape
    heads = width // HEAD_DIM
    spans = rows // SPAN
    groups = heads // per
    half_width = heads * tp_size // 2 * HEAD_DIM
    members = 2 * inner_size
    own_heads = heads // members
    tiles = columns // tile
    pieces = columns // weight_tile
    near = hi_size // 2 * per * HEAD_DIM
    away = half_width - near
    hi, lo, inner, tp = (lax.axis_index(a) for a in ("hi", "lo", "inner", "tp"))
    member = lo * inner_size + inner
    strides = []
    by = tp_size // 2
    while by >= 1:
        strides.append(by)
        by //= 2

    def member_at(index):
        return {"lo": index // inner_size, "inner": index % inner_size}

    def flipped(index, by):
        return index + by - 2 * by * ((index // by) % 2)

    def remote(source, target, send, recv, device):
        return pltpu.make_async_remote_copy(
            src_ref=source,
            dst_ref=target,
            send_sem=send,
            recv_sem=recv,
            device_id=device,
            device_id_type=MESH_ID,
        )

    def span_rows(span):
        return pl.ds(span * SPAN, SPAN)

    def lanes_of(head):
        return pl.ds(pl.multiple_of(head * HEAD_DIM, HEAD_DIM), HEAD_DIM)

    def slot_rows(block_hi, block_inner):
        return pl.ds(pl.multiple_of((block_hi * inner_size + block_inner) * depth, depth), depth)

    loads = [
        pltpu.make_async_copy(source, target, load_sems.at[number])
        for number, (source, target) in enumerate(
            (
                (forget_in, forget_ref),
                (value_in, value_ref),
                (weight_in, whole_weight.at[slot_rows(hi, inner)]),
                (query_in, query_ref),
                (gate_in, gate_ref),
            )
        )
    ]
    for load in loads:
        load.start()

    barrier = pltpu.get_barrier_semaphore()

    peers = members - 1 + tp_size - 1
    for step in range(1, members):
        pl.semaphore_signal(
            barrier,
            inc=1,
            device_id=member_at((member + step) % members),
            device_id_type=MESH_ID,
        )
    for step in range(1, tp_size):
        pl.semaphore_signal(
            barrier, inc=1, device_id={"tp": (tp + step) % tp_size}, device_id_type=MESH_ID
        )
    for step in (1, -1):
        there = hi + step
        inside = (there >= 0) & (there < hi_size)

        @pl.when(inside)
        def _():
            pl.semaphore_signal(barrier, inc=1, device_id={"hi": there}, device_id_type=MESH_ID)

        peers = peers + jnp.where(inside, 1, 0)
    pl.semaphore_wait(barrier, peers)

    def weight_block(block_hi, block_inner, piece):
        return whole_weight.at[
            slot_rows(block_hi, block_inner), pl.ds(piece * weight_tile, weight_tile)
        ]

    def step_of(way):
        return 1 if way == 0 else -1

    def line_copy(way, hop, piece):
        block = weight_block(hi - step_of(way) * (hop - 1), inner, piece)
        return remote(
            block,
            block,
            line_sems.at[0, way, hop - 1, piece],
            line_sems.at[1, way, hop - 1, piece],
            {"hi": hi + step_of(way)},
        )

    def sends(way, hop):
        origin = hi - step_of(way) * (hop - 1)
        target = hi + step_of(way)
        return (origin >= 0) & (origin < hi_size) & (target >= 0) & (target < hi_size)

    def receives(way, hop):
        origin = hi - step_of(way) * hop
        return (origin >= 0) & (origin < hi_size)

    def side_copy(reach, block_hi, piece):
        block = weight_block(block_hi, inner, piece)
        return remote(
            block,
            block,
            side_sems.at[0, reach - 1, block_hi, piece],
            side_sems.at[1, reach - 1, block_hi, piece],
            {"inner": (inner + reach) % inner_size},
        )

    def start_line(way, piece):
        @pl.when(sends(way, 1))
        def _():
            line_copy(way, 1, piece).start()

    def start_side(piece):
        for reach in range(1, inner_size):
            side_copy(reach, hi, piece).start()

    def take_hop(hop, way, piece):
        if hop >= hi_size:
            return

        @pl.when(receives(way, hop))
        def _():
            line_copy(way, hop, piece).wait_recv()
            for reach in range(1, inner_size):
                side_copy(reach, hi - step_of(way) * hop, piece).start()

        if hop + 1 < hi_size:

            @pl.when(sends(way, hop + 1))
            def _():
                line_copy(way, hop + 1, piece).start()

    near_first = hi < hi_size // 2
    near_block = jnp.where(near_first, 0, hi_size - hi_size // 2)
    away_block = jnp.where(near_first, hi_size // 2, 0)
    block_depth = per * HEAD_DIM

    def take_near_sides():
        for reach in range(1, inner_size):
            for number in range(hi_size // 2):
                for piece in range(pieces):
                    side_copy(reach, near_block + number, piece).wait_recv()

    def take_away_sides(piece):
        for reach in range(1, inner_size):
            for number in range(hi_size - hi_size // 2):
                side_copy(reach, away_block + number, piece).wait_recv()

    def state_copy(head):
        return remote(
            state_out.at[head],
            gathered.at[member, head % own_heads],
            gather_send.at[head],
            gather_recv.at[member, head % own_heads],
            member_at(head // own_heads),
        )

    def state_arrival(index, number):
        return remote(
            state_out.at[0],
            gathered.at[index, number],
            gather_send.at[0],
            gather_recv.at[index, number],
            member_at(index),
        )

    def chain_copy(number):
        return remote(
            chain_out.at[number],
            chain_in.at[number],
            chain_sems.at[0, number],
            chain_sems.at[1, number],
            {"hi": hi + 1},
        )

    def deliver_copy(index, number):
        head = member * own_heads + number
        return remote(
            deliver_out.at[index, number],
            carried.at[head],
            deliver_send.at[index, number],
            deliver_recv.at[head],
            member_at(index),
        )

    def deliver_arrival(head):
        return remote(
            deliver_out.at[0, 0],
            carried.at[head],
            deliver_send.at[0, 0],
            deliver_recv.at[head],
            member_at(head // own_heads),
        )

    def state_body(turn, carry):
        head = (turn + (member + 1) * own_heads) % heads
        causal = lower_triangle()
        gap = gap_ref[pl.ds(tp * heads + head, 1), :]
        lanes = lanes_of(head)
        this_head = lax.broadcasted_iota(jnp.int32, (heads, SPAN), 0) == head
        state = jnp.zeros((HEAD_DIM, HEAD_DIM), jnp.float32)
        base = jnp.zeros((1, HEAD_DIM), jnp.float32)
        for span in range(spans):
            part = span_rows(span)
            surge = jnp.sum(jnp.where(this_head, surge_ref[:, part], 0.0), axis=0, keepdims=True)
            keys, running = decays(forget_ref[part, lanes], gap, surge, causal)
            keys_ref[part, lanes] = keys
            running_ref[part, lanes] = running
            base_ref[head, span : span + 1, :] = base
            if span > 0:
                starts_ref[head, span - 1] = state.astype(jnp.bfloat16)
            ending = running[SPAN - 1 : SPAN, :]
            kept = (keys * jnp.exp(ending - running)).astype(jnp.bfloat16)
            state = state * jnp.exp(ending) + dot(value_ref[part, lanes], kept, TN)
            base = base + ending
        decay = jnp.exp(base)
        high = decay.astype(jnp.bfloat16).astype(jnp.float32)
        first = lax.broadcasted_iota(jnp.int32, (TAIL, HEAD_DIM), 0) == 0
        item = state.astype(jnp.bfloat16)
        tail = jnp.where(first, high, decay - high).astype(jnp.bfloat16)
        state_out[head, 0:HEAD_DIM, :] = item
        state_out[head, HEAD_DIM:, :] = tail
        owner = head // own_heads

        @pl.when(owner == member)
        def _():
            gathered[member, head % own_heads, 0:HEAD_DIM, :] = item
            gathered[member, head % own_heads, HEAD_DIM:, :] = tail

        @pl.when(owner != member)
        def _():
            state_copy(head).start()

        return carry

    def chain_states():
        @pl.when(hi == 0)
        def _():
            chain_in[...] = jnp.zeros_like(chain_in)

        def body(number, carry):
            for index in range(members):

                @pl.when(member != index)
                def _():
                    state_arrival(index, number).wait_recv()

            @pl.when(hi > 0)
            def _():
                chain_copy(number).wait_recv()

            state = chain_in[number].astype(jnp.float32)
            for index in range(members):
                deliver_out[index, number] = state.astype(jnp.bfloat16)
                tail = gathered[index, number, HEAD_DIM:, :].astype(jnp.float32)
                item = gathered[index, number, 0:HEAD_DIM, :].astype(jnp.float32)
                state = state * (tail[0:1, :] + tail[1:2, :]) + item
            chain_out[number] = state.astype(jnp.bfloat16)

            @pl.when(hi + 1 < hi_size)
            def _():
                chain_copy(number).start()

            for index in range(members):

                @pl.when(member != index)
                def _():
                    deliver_copy(index, number).start()

            carried[member * own_heads + number] = deliver_out[member, number]
            return carry

        lax.fori_loop(0, own_heads, body, 0)

    def take_states():
        def body(head, carry):
            @pl.when(head // own_heads != member)
            def _():
                deliver_arrival(head).wait_recv()

            return carry

        lax.fori_loop(0, heads, body, 0)

    gain = gain_ref[...]

    def local_body(head, carry):
        causal = lower_triangle()
        lanes = lanes_of(head)
        middle = SPAN // 2
        for span in range(spans):
            part = span_rows(span)
            running = running_ref[part, lanes]
            anchor = running[middle - 1 : middle, :]
            queries = silu(query_ref[part, lanes].astype(jnp.float32)) * (HEAD_DIM**-0.5)
            reach = queries * jnp.exp(running - anchor)
            back = keys_ref[part, lanes] * jnp.exp(anchor - running)
            scores = dot(reach.astype(jnp.bfloat16), back.astype(jnp.bfloat16), NT)
            scores = jnp.where(causal, scores, 0.0).astype(jnp.bfloat16)
            out = dot(scores, value_ref[part, lanes])
            if span > 0:
                out = out + dot(
                    (reach * jnp.exp(anchor)).astype(jnp.bfloat16), starts_ref[head, span - 1], NT
                )
            local_ref[part, lanes] = out
            base = base_ref[head, span : span + 1, :]
            reach_ref[part, lanes] = (reach * jnp.exp(anchor + base)).astype(jnp.bfloat16)
            gated_ref[part, lanes] = gain * silu(gate_ref[part, lanes].astype(jnp.float32))
        return carry

    def keeps(index, group):
        return (index * groups + group) % 2 == lo

    def group_lanes(index, group, which):
        start = which * half_width + (index * groups + group) // 2 * per * HEAD_DIM
        return pl.ds(pl.multiple_of(start, HEAD_DIM), per * HEAD_DIM)

    def swap_copy(group, span):
        start = 2 * half_width + group * per * HEAD_DIM
        return remote(
            mixed_ref.at[span_rows(span), pl.ds(start, per * HEAD_DIM)],
            mixed_ref.at[span_rows(span), group_lanes(tp, group, 1)],
            swap_sems.at[0, group, span],
            swap_sems.at[1, group, span],
            {"lo": 1 - lo},
        )

    def origin_of(index, mask):
        for bit, by in enumerate(strides):
            if (mask >> bit) & 1:
                index = flipped(index, by)
        return index

    def tp_copy(stage, which, mask, group, span):
        block = mixed_ref.at[span_rows(span), group_lanes(origin_of(tp, mask), group, which)]
        return remote(
            block,
            block,
            tp_sems.at[0, stage, which, mask, group, span],
            tp_sems.at[1, stage, which, mask, group, span],
            {"tp": flipped(tp, strides[stage])},
        )

    def mix(span):
        part = span_rows(span)
        for head in range(heads):
            lanes = lanes_of(head)
            out = local_ref[part, lanes] + dot(reach_ref[part, lanes], carried[head], NT)
            mean_sq = jnp.mean(out * out, axis=1, keepdims=True)
            mixed = out * lax.rsqrt(mean_sq + EPSILON) * gated_ref[part, lanes]
            group = head // per
            kept_start = (tp * groups + group) // 2 * per * HEAD_DIM + head % per * HEAD_DIM
            away_start = 2 * half_width + head * HEAD_DIM
            start = jnp.where(keeps(tp, group), kept_start, away_start)
            mixed_ref[part, pl.ds(pl.multiple_of(start, HEAD_DIM), HEAD_DIM)] = mixed.astype(
                jnp.bfloat16
            )

    def send_away(span):
        for group in range(groups):

            @pl.when(jnp.logical_not(keeps(tp, group)))
            def _():
                swap_copy(group, span).start()

    def send_kept(span):
        for group in range(groups):

            @pl.when(keeps(tp, group))
            def _():
                for stage in range(len(strides)):
                    tp_copy(stage, 0, 0, group, span).start()

    def take_swap(span):
        for group in range(groups):

            @pl.when(keeps(tp, group))
            def _():
                swap_copy(group, span).wait_recv()
                for stage in range(len(strides)):
                    tp_copy(stage, 1, 0, group, span).start()

    def take_stage(stage, which, span):
        peer = flipped(tp, strides[stage])
        for mask in range(1 << stage):
            for group in range(groups):

                @pl.when(keeps(origin_of(peer, mask), group))
                def _():
                    tp_copy(stage, which, mask, group, span).wait_recv()
                    for later in range(stage + 1, len(strides)):
                        tp_copy(later, which, mask | (1 << stage), group, span).start()

    def partial_copy(piece, span):
        return remote(
            partial_out.at[piece, span],
            partial_in.at[piece, span],
            partial_sems.at[0, piece, span],
            partial_sems.at[1, piece, span],
            {"lo": 1 - lo},
        )

    def both(span, start, depth):
        part = span_rows(span)
        start = pl.multiple_of(start, HEAD_DIM)
        later = pl.multiple_of(start + half_width, HEAD_DIM)
        return jnp.concatenate(
            [mixed_ref[part, pl.ds(later, depth)], mixed_ref[part, pl.ds(start, depth)]], axis=0
        )

    def multiply_near(span):
        start = near_block * block_depth
        left = both(span, start, near)
        rows_near = pl.ds(pl.multiple_of(start, HEAD_DIM), near)
        for number in range(tiles):
            lanes = pl.ds(number * tile, tile)
            total_ref[span, :, lanes] = dot(left, whole_weight[rows_near, lanes])

    def multiply_away(piece):
        start = away_block * block_depth
        rows_away = pl.ds(pl.multiple_of(start, HEAD_DIM), away)
        lanes = pl.ds(piece * weight_tile, weight_tile)
        right = whole_weight[rows_away, lanes]
        for span in range(spans):
            total = total_ref[span, :, lanes] + dot(both(span, start, away), right)
            partial_out[piece, span] = total[0:SPAN].astype(jnp.bfloat16)
            partial_copy(piece, span).start()
            total_ref[span, SPAN:, lanes] = total[SPAN:]

    def square_copy(step, span):
        return remote(
            squares_ref.at[tp, span],
            squares_ref.at[tp, span],
            square_send.at[step - 1, span],
            square_recv.at[step - 1, span],
            {"tp": (tp + step) % tp_size},
        )

    def combine(piece, span):
        lanes = pl.ds(piece * weight_tile, weight_tile)
        partial_copy(piece, span).wait_recv()
        total = total_ref[span, SPAN:, lanes] + partial_in[piece, span].astype(jnp.float32)
        rounded = total.astype(jnp.bfloat16)
        projected_ref[span_rows(span), lanes] = rounded
        branch = rounded.astype(jnp.float32)
        branch = branch * branch
        squares = branch[:, 0:HEAD_DIM]
        for start in range(HEAD_DIM, weight_tile, HEAD_DIM):
            squares = squares + branch[:, start : start + HEAD_DIM]
        if piece > 0:
            squares = squares + sums_ref[span]
        sums_ref[span] = squares

    def share_squares(span):
        column = jnp.sum(sums_ref[span], axis=1, keepdims=True)
        row = jnp.sum(jnp.where(diagonal(), column, 0.0), axis=0, keepdims=True)
        squares_ref[tp, span] = jnp.broadcast_to(row, (8, HEAD_DIM))
        for step in range(1, tp_size):
            square_copy(step, span).start()

    def store_copy(piece):
        lanes = pl.ds(piece * weight_tile, weight_tile)
        return pltpu.make_async_copy(
            projected_ref.at[:, lanes], projected_hbm.at[:, lanes], store_sems.at[piece]
        )

    def finish(span):
        for step in range(1, tp_size):
            square_copy(step, span).wait_recv()
        total = squares_ref[0, span, 0:1, :]
        for index in range(1, tp_size):
            total = total + squares_ref[index, span, 0:1, :]
        scale_ref[span : span + 1, :] = lax.rsqrt(total * (1.0 / (columns * tp_size)) + EPSILON)

    def line_sent(first, last):
        for hop in range(first, last):
            for piece in range(pieces):
                for way in (0, 1):

                    @pl.when(sends(way, hop))
                    def _():
                        line_copy(way, hop, piece).wait_send()

    def states_sent():
        def body(head, carry):
            @pl.when(head // own_heads != member)
            def _():
                state_copy(head).wait_send()

            return carry

        lax.fori_loop(0, heads, body, 0)
        for number in range(own_heads):

            @pl.when(hi + 1 < hi_size)
            def _():
                chain_copy(number).wait_send()

            for index in range(members):

                @pl.when(member != index)
                def _():
                    deliver_copy(index, number).wait_send()

    def mixed_sent(span):
        for group in range(groups):

            @pl.when(jnp.logical_not(keeps(tp, group)))
            def _():
                swap_copy(group, span).wait_send()

            for stage in range(len(strides)):
                for which in (0, 1):
                    for mask in range(1 << stage):

                        @pl.when(keeps(origin_of(tp, mask), group))
                        def _():
                            tp_copy(stage, which, mask, group, span).wait_send()

    early = hi < hi_size // 2
    scope = jax.named_scope

    def local():
        with scope("local"):
            lax.fori_loop(0, heads, local_body, 0)

    def hop_pieces(hop, way, first, last):
        with scope(f"hop{hop}_{way}_{first}"):
            for piece in range(first, last):
                take_hop(hop, way, piece)

    loads[2].wait()
    for piece in range(pieces):
        if piece < 3:
            start_line(0, piece)
        elif piece < 5:

            @pl.when(hi + 2 >= piece)
            def _():
                start_line(0, piece)

        start_line(1, piece)
    for piece in range(pieces):
        start_side(piece)
    loads[0].wait()
    loads[1].wait()
    with scope("state"):
        lax.fori_loop(0, heads, state_body, 0)
    loads[3].wait()
    loads[4].wait()

    @pl.when(jnp.logical_not(early))
    def _():
        local()

    with scope("chain"):
        chain_states()
    for piece in range(3, pieces):
        if piece < 5:

            @pl.when(hi + 2 < piece)
            def _():
                start_line(0, piece)

        else:
            start_line(0, piece)

    @pl.when(early)
    def _():
        local()

    with scope("take_states"):
        take_states()
    with scope("mix"):
        for span in range(spans):
            mix(span)
            send_away(span)
            if span < 2:
                send_kept(span)
    hop_pieces(1, 1, 0, 6)
    with scope("swap01"):
        for span in range(2):
            take_swap(span)
            send_kept(span + 2)
    hop_pieces(1, 1, 6, 8)
    hop_pieces(1, 0, 0, 4)

    def take_rest(span):
        with scope(f"take{span}"):
            for stage in range(1, len(strides)):
                for which in (0, 1):
                    take_stage(stage, which, span)

    with scope("y0"):
        take_stage(0, 0, 0)
        take_swap(2)
        take_stage(0, 0, 1)
        take_stage(0, 1, 0)
    hop_pieces(1, 0, 4, 8)
    hop_pieces(2, 1, 0, 3)
    def near_part(span):
        if hi_size <= 4:
            take_rest(span)
            if span == 0:
                take_near_sides()
            with scope(f"near{span}"):
                multiply_near(span)

    near_part(0)
    with scope("y1"):
        take_swap(3)
        take_stage(0, 0, 2)
        take_stage(0, 1, 1)
        take_stage(0, 0, 3)
    hop_pieces(2, 1, 3, 5)
    hop_pieces(2, 0, 0, 3)
    near_part(1)
    with scope("y2"):
        take_stage(0, 1, 2)
        take_stage(0, 1, 3)
    near_part(2)
    near_part(3)
    hop_pieces(2, 1, 5, 8)
    hop_pieces(2, 0, 3, 8)
    if hi_size > 4:
        for hop in range(3, hi_size - 1):
            for way in (0, 1):
                hop_pieces(hop, way, 0, pieces)
        take_near_sides()
        for span in range(spans):
            take_rest(span)
            multiply_near(span)
    for piece in range(pieces):
        with scope(f"far_wait{piece}"):
            if hi_size > 3:
                for way in (0, 1):
                    take_hop(hi_size - 1, way, piece)
            take_away_sides(piece)
        with scope(f"far{piece}"):
            multiply_away(piece)
        with scope(f"sent{piece}"):
            if piece == 0:
                states_sent()
            if piece < spans:
                mixed_sent(piece)
            if piece == pieces - 3:
                line_sent(1, 2)
            if piece == pieces - 2:
                line_sent(2, min(3, hi_size))
            if piece == pieces - 1:
                line_sent(3, hi_size)
        if piece > 0:
            with scope(f"combine{piece - 1}"):
                for span in range(spans):
                    combine(piece - 1, span)
                store_copy(piece - 1).start()
    with scope("combine_last"):
        for span in range(spans):
            combine(pieces - 1, span)
            share_squares(span)
        store_copy(pieces - 1).start()
    with scope("finish"):
        for span in range(spans):
            finish(span)
        scale_copy = pltpu.make_async_copy(scale_ref, scale_hbm, store_sems.at[pieces])
        scale_copy.start()
    with scope("drain"):
        for piece in range(pieces):
            for reach in range(1, inner_size):
                for block_hi in range(hi_size):
                    side_copy(reach, block_hi, piece).wait_send()
            for span in range(spans):
                partial_copy(piece, span).wait_send()
            store_copy(piece).wait()
        for span in range(spans):
            for step in range(1, tp_size):
                square_copy(step, span).wait_send()
        scale_copy.wait()


def layer(sizes, arrays):
    hi_size, inner_size, tp_size, per, tile, weight_tile = sizes
    rows, width = arrays[0].shape
    depth, columns = arrays[7].shape
    heads = width // HEAD_DIM
    groups = heads // per
    spans = rows // SPAN
    members = 2 * inner_size
    own_heads = heads // members
    stages = tp_size.bit_length() - 1
    half_width = heads * tp_size // 2 * HEAD_DIM
    pieces = columns // weight_tile
    vmem = pl.BlockSpec(memory_space=pltpu.VMEM)
    anywhere = pl.BlockSpec(memory_space=pl.ANY)
    item = (HEAD_DIM + TAIL, HEAD_DIM)
    square = (HEAD_DIM, HEAD_DIM)
    bf16, f32 = jnp.bfloat16, jnp.float32
    dma = pltpu.SemaphoreType.DMA
    return pl.pallas_call(
        functools.partial(layer_kernel, sizes),
        in_specs=[anywhere] * 4 + [vmem] * 3 + [anywhere],
        out_specs=[anywhere, anywhere],
        out_shape=[
            jax.ShapeDtypeStruct((rows, columns), bf16),
            jax.ShapeDtypeStruct((spans, HEAD_DIM), f32),
        ],
        scratch_shapes=[
            pltpu.VMEM((hi_size * inner_size * depth, columns), bf16),
            pltpu.VMEM((rows, width), bf16),
            pltpu.VMEM((rows, width), bf16),
            pltpu.VMEM((rows, width), bf16),
            pltpu.VMEM((rows, width), bf16),
            pltpu.VMEM((rows, width), f32),
            pltpu.VMEM((rows, width), f32),
            pltpu.VMEM((heads, max(8, spans), HEAD_DIM), f32),
            pltpu.VMEM((heads, max(1, spans - 1)) + square, bf16),
            pltpu.VMEM((heads,) + item, bf16),
            pltpu.VMEM((members, own_heads) + item, bf16),
            pltpu.VMEM((own_heads,) + square, bf16),
            pltpu.VMEM((own_heads,) + square, bf16),
            pltpu.VMEM((members, own_heads) + square, bf16),
            pltpu.VMEM((heads,) + square, bf16),
            pltpu.VMEM((rows, width), f32),
            pltpu.VMEM((rows, width), bf16),
            pltpu.VMEM((rows, width), f32),
            pltpu.VMEM((rows, 2 * half_width + width), bf16),
            pltpu.VMEM((pieces, spans, SPAN, weight_tile), bf16),
            pltpu.VMEM((pieces, spans, SPAN, weight_tile), bf16),
            pltpu.VMEM((spans, 2 * SPAN, columns), f32),
            pltpu.VMEM((rows, columns), bf16),
            pltpu.VMEM((spans, SPAN, HEAD_DIM), f32),
            pltpu.VMEM((tp_size, spans, 8, HEAD_DIM), f32),
            pltpu.VMEM((spans, HEAD_DIM), f32),
            dma((5,)),
            dma((heads,)),
            dma((members, own_heads)),
            dma((2, own_heads)),
            dma((members, own_heads)),
            dma((heads,)),
            dma((2, groups, spans)),
            dma((2, stages, 2, tp_size // 2, groups, spans)),
            dma((2, 2, max(1, hi_size - 1), pieces)),
            dma((2, max(1, inner_size - 1), hi_size, pieces)),
            dma((2, pieces, spans)),
            dma((tp_size - 1, spans)),
            dma((tp_size - 1, spans)),
            dma((pieces + 1,)),
        ],
        name="layer",
        compiler_params=pltpu.CompilerParams(
            collective_id=0, has_side_effects=True, vmem_limit_bytes=60000 * 1024
        ),
        cost_estimate=pl.CostEstimate(
            flops=rows * width * 10000, bytes_accessed=14 * rows * width, transcendentals=0
        ),
    )(*arrays)


def per_device(hi_size, inner_size, tp_size, *arrays):
    query, forget, value, gate, gap, surge, head_gain, matrix, branch_gain, residual = arrays
    per = inner_size * matrix.shape[0] // HEAD_DIM
    projected, scale = layer(
        (hi_size, inner_size, tp_size, per, 256, 128),
        (
            query,
            forget,
            value,
            gate,
            gap.reshape(-1, HEAD_DIM),
            surge,
            head_gain.reshape(1, HEAD_DIM),
            matrix,
        ),
    )
    columns = matrix.shape[1]
    gain_part = lax.dynamic_slice_in_dim(branch_gain, lax.axis_index("tp") * columns, columns)
    branch = projected.astype(jnp.float32) * scale.reshape(-1)[:, None] * gain_part
    return (residual.astype(jnp.float32) + branch).astype(jnp.bfloat16)


def solution(mesh):
    sp_size, tp_size = mesh.shape["sp"], mesh.shape["tp"]
    sp = ("hi", "lo", "inner")
    placed = (
        P(sp, "tp"),
        P(sp, "tp"),
        P(sp, "tp"),
        P(sp, "tp"),
        P(),
        P("tp", sp),
        P(),
        P(sp, "tp"),
        P(),
        P(sp, "tp"),
    )

    def whole(*arrays):
        inner = max(1, HEAD_DIM * sp_size // arrays[7].shape[0])
        hi = sp_size // (2 * inner)
        devices = mesh.devices.reshape(hi, 2, inner, tp_size)
        paired = Mesh(devices, ("hi", "lo", "inner", "tp"))
        return jax.shard_map(
            functools.partial(per_device, hi, inner, tp_size),
            mesh=paired,
            in_specs=placed,
            out_specs=P(sp, "tp"),
            check_vma=False,
        )(*arrays)

    return whole
```

```python
import functools

import jax
import jax.numpy as jnp
from jax import lax
from jax.experimental import pallas as pl
from jax.experimental.pallas import tpu as pltpu
from jax.sharding import Mesh
from jax.sharding import PartitionSpec as P

HEAD_DIM = 128
SPAN = 128
TAIL = 16
EPSILON = 1e-06
NT = (((1,), (1,)), ((), ()))
TN = (((0,), (0,)), ((), ()))
NN = (((1,), (0,)), ((), ()))
MESH_ID = pl.DeviceIdType.MESH


def dot(a, b, dims=NN):
    return lax.dot_general(a, b, dims, preferred_element_type=jnp.float32)


def lower_triangle():
    rows = lax.broadcasted_iota(jnp.int32, (SPAN, SPAN), 0)
    columns = lax.broadcasted_iota(jnp.int32, (SPAN, SPAN), 1)
    return rows >= columns


def diagonal():
    rows = lax.broadcasted_iota(jnp.int32, (SPAN, SPAN), 0)
    columns = lax.broadcasted_iota(jnp.int32, (SPAN, SPAN), 1)
    return rows == columns


def silu(logits):
    return logits / (1.0 + jnp.exp(-logits))


def decays(logits, gap, surge, causal):
    keys = gap / (1.0 + jnp.exp(logits.astype(jnp.float32)))
    series = keys * (1.0 / 7.0) + (1.0 / 6.0)
    for order in (5, 4, 3, 2):
        series = series * keys + (1.0 / order)
    logs = -(series * keys + 1.0) * keys
    high = logs.astype(jnp.bfloat16)
    low = (logs - high.astype(jnp.float32)).astype(jnp.bfloat16)
    ones = causal.astype(jnp.bfloat16)
    surged = jnp.sum(jnp.where(causal, surge, 0.0), axis=1, keepdims=True)
    return keys, dot(ones, high) + dot(ones, low) + surged


def layer_kernel(
    sizes,
    query_in,
    forget_in,
    value_in,
    gate_in,
    gap_ref,
    surge_ref,
    gain_ref,
    weight_in,
    projected_ref,
    scale_ref,
    whole_weight,
    query_ref,
    forget_ref,
    value_ref,
    gate_ref,
    running_ref,
    keys_ref,
    base_ref,
    starts_ref,
    state_out,
    gathered,
    chain_in,
    chain_out,
    deliver_out,
    carried,
    local_ref,
    reach_ref,
    gated_ref,
    mixed_ref,
    partial_out,
    partial_in,
    total_ref,
    sums_ref,
    squares_ref,
    load_sems,
    gather_send,
    gather_recv,
    chain_send,
    chain_recv,
    deliver_send,
    deliver_recv,
    swap_send,
    swap_recv,
    tp_send,
    tp_recv,
    line_send,
    line_recv,
    side_sems,
    partial_send,
    partial_recv,
    square_send,
    square_recv,
):
    hi_size, inner_size, tp_size, per, tile, weight_tile = sizes
    rows, width = query_in.shape
    depth, columns = weight_in.shape
    heads = width // HEAD_DIM
    spans = rows // SPAN
    groups = heads // per
    half_width = heads * tp_size // 2 * HEAD_DIM
    members = 2 * inner_size
    own_heads = heads // members
    tiles = columns // tile
    pieces = columns // weight_tile
    near = hi_size // 2 * per * HEAD_DIM
    away = half_width - near
    hi, lo, inner, tp = (lax.axis_index(a) for a in ("hi", "lo", "inner", "tp"))
    member = lo * inner_size + inner
    strides = []
    by = tp_size // 2
    while by >= 1:
        strides.append(by)
        by //= 2

    def member_at(index):
        return {"lo": index // inner_size, "inner": index % inner_size}

    def flipped(index, by):
        return index + by - 2 * by * ((index // by) % 2)

    def remote(source, target, send, recv, device):
        return pltpu.make_async_remote_copy(
            src_ref=source,
            dst_ref=target,
            send_sem=send,
            recv_sem=recv,
            device_id=device,
            device_id_type=MESH_ID,
        )

    def span_rows(span):
        return pl.ds(span * SPAN, SPAN)

    def lanes_of(head):
        return pl.ds(pl.multiple_of(head * HEAD_DIM, HEAD_DIM), HEAD_DIM)

    def slot_rows(block_hi, block_inner):
        return pl.ds(pl.multiple_of((block_hi * inner_size + block_inner) * depth, depth), depth)

    loads = [
        pltpu.make_async_copy(source, target, load_sems.at[number])
        for number, (source, target) in enumerate(
            (
                (weight_in, whole_weight.at[slot_rows(hi, inner)]),
                (forget_in, forget_ref),
                (value_in, value_ref),
                (query_in, query_ref),
                (gate_in, gate_ref),
            )
        )
    ]
    for load in loads:
        load.start()

    barrier = pltpu.get_barrier_semaphore()

    peers = members - 1 + tp_size - 1
    for step in range(1, members):
        pl.semaphore_signal(
            barrier,
            inc=1,
            device_id=member_at((member + step) % members),
            device_id_type=MESH_ID,
        )
    for step in range(1, tp_size):
        pl.semaphore_signal(
            barrier, inc=1, device_id={"tp": (tp + step) % tp_size}, device_id_type=MESH_ID
        )
    for step in (1, -1):
        there = hi + step
        inside = (there >= 0) & (there < hi_size)

        @pl.when(inside)
        def _():
            pl.semaphore_signal(barrier, inc=1, device_id={"hi": there}, device_id_type=MESH_ID)

        peers = peers + jnp.where(inside, 1, 0)
    pl.semaphore_wait(barrier, peers)

    def weight_block(block_hi, block_inner, piece):
        return whole_weight.at[
            slot_rows(block_hi, block_inner), pl.ds(piece * weight_tile, weight_tile)
        ]

    def step_of(way):
        return 1 if way == 0 else -1

    def line_copy(way, hop, piece):
        block = weight_block(hi - step_of(way) * (hop - 1), inner, piece)
        return remote(
            block,
            block,
            line_send.at[way, hop - 1],
            line_recv.at[hi - step_of(way) * (hop - 1), piece],
            {"hi": hi + step_of(way)},
        )

    def line_arrival(origin, piece):
        block = weight_block(origin, inner, piece)
        return remote(block, block, line_send.at[0, 0], line_recv.at[origin, piece], {"hi": origin})

    def line_sent(way, hop):
        block = whole_weight.at[slot_rows(0, 0)]
        return remote(
            block, block, line_send.at[way, hop - 1], line_recv.at[0, 0], {"hi": hi + step_of(way)}
        )

    def sends(way, hop):
        origin = hi - step_of(way) * (hop - 1)
        target = hi + step_of(way)
        return (origin >= 0) & (origin < hi_size) & (target >= 0) & (target < hi_size)

    def receives(way, hop):
        origin = hi - step_of(way) * hop
        return (origin >= 0) & (origin < hi_size)

    def side_copy(reach, block_hi, piece):
        block = weight_block(block_hi, inner, piece)
        return remote(
            block,
            block,
            side_sems.at[0, reach - 1, block_hi, piece],
            side_sems.at[1, reach - 1, block_hi, piece],
            {"inner": (inner + reach) % inner_size},
        )

    def start_line(way, piece):
        @pl.when(sends(way, 1))
        def _():
            line_copy(way, 1, piece).start()

    def start_side(piece):
        for reach in range(1, inner_size):
            side_copy(reach, hi, piece).start()

    def take_hop(hop, way, piece):
        if hop >= hi_size:
            return

        @pl.when(receives(way, hop))
        def _():
            line_arrival(hi - step_of(way) * hop, piece).wait_recv()
            for reach in range(1, inner_size):
                side_copy(reach, hi - step_of(way) * hop, piece).start()

        if hop + 1 < hi_size:

            @pl.when(sends(way, hop + 1))
            def _():
                line_copy(way, hop + 1, piece).start()

    near_first = hi < hi_size // 2
    near_block = jnp.where(near_first, 0, hi_size - hi_size // 2)
    away_block = jnp.where(near_first, hi_size // 2, 0)
    block_depth = per * HEAD_DIM

    def take_near_sides():
        for reach in range(1, inner_size):
            for number in range(hi_size // 2):
                for piece in range(pieces):
                    side_copy(reach, near_block + number, piece).wait_recv()

    def take_away_sides(piece):
        for reach in range(1, inner_size):
            for number in range(hi_size - hi_size // 2):
                side_copy(reach, away_block + number, piece).wait_recv()

    def state_copy(head):
        return remote(
            state_out.at[head],
            gathered.at[member, head % own_heads],
            gather_send.at[0],
            gather_recv.at[member, head % own_heads],
            member_at(head // own_heads),
        )

    def state_arrival(index, number):
        return remote(
            state_out.at[0],
            gathered.at[index, number],
            gather_send.at[0],
            gather_recv.at[index, number],
            member_at(index),
        )

    def chain_copy(number):
        return remote(
            chain_out.at[number],
            chain_in.at[number],
            chain_send.at[0],
            chain_recv.at[number],
            {"hi": hi + 1},
        )

    def deliver_copy(index, number):
        head = member * own_heads + number
        return remote(
            deliver_out.at[index * own_heads + number],
            carried.at[head],
            deliver_send.at[0],
            deliver_recv.at[head],
            member_at(index),
        )

    def deliver_arrival(head):
        return remote(
            deliver_out.at[0],
            carried.at[head],
            deliver_send.at[0],
            deliver_recv.at[head],
            member_at(head // own_heads),
        )

    def state_body(turn, carry):
        head = (turn + (member + 1) * own_heads) % heads
        causal = lower_triangle()
        gap = gap_ref[pl.ds(tp * heads + head, 1), :]
        lanes = lanes_of(head)
        this_head = lax.broadcasted_iota(jnp.int32, (heads, SPAN), 0) == head
        state = jnp.zeros((HEAD_DIM, HEAD_DIM), jnp.float32)
        base = jnp.zeros((1, HEAD_DIM), jnp.float32)
        for span in range(spans):
            part = span_rows(span)
            surge = jnp.sum(jnp.where(this_head, surge_ref[:, part], 0.0), axis=0, keepdims=True)
            keys, running = decays(forget_ref[part, lanes], gap, surge, causal)
            keys_ref[part, lanes] = keys
            running_ref[part, lanes] = running
            base_ref[head, span : span + 1, :] = base
            if span > 0:
                starts_ref[head, span - 1] = state.astype(jnp.bfloat16)
            ending = running[SPAN - 1 : SPAN, :]
            kept = (keys * jnp.exp(ending - running)).astype(jnp.bfloat16)
            state = state * jnp.exp(ending) + dot(value_ref[part, lanes], kept, TN)
            base = base + ending
        decay = jnp.exp(base)
        high = decay.astype(jnp.bfloat16).astype(jnp.float32)
        first = lax.broadcasted_iota(jnp.int32, (TAIL, HEAD_DIM), 0) == 0
        item = state.astype(jnp.bfloat16)
        tail = jnp.where(first, high, decay - high).astype(jnp.bfloat16)
        state_out[head, 0:HEAD_DIM, :] = item
        state_out[head, HEAD_DIM:, :] = tail
        owner = head // own_heads

        @pl.when(owner == member)
        def _():
            gathered[member, head % own_heads, 0:HEAD_DIM, :] = item
            gathered[member, head % own_heads, HEAD_DIM:, :] = tail

        @pl.when(owner != member)
        def _():
            state_copy(head).start()

        return carry

    def chain_states():
        @pl.when(hi == 0)
        def _():
            chain_in[...] = jnp.zeros_like(chain_in)

        def body(number, carry):
            for index in range(members):

                @pl.when(member != index)
                def _():
                    state_arrival(index, number).wait_recv()

            @pl.when(hi > 0)
            def _():
                chain_copy(number).wait_recv()

            state = chain_in[number].astype(jnp.float32)
            for index in range(members):
                deliver_out[index * own_heads + number] = state.astype(jnp.bfloat16)
                tail = gathered[index, number, HEAD_DIM:, :].astype(jnp.float32)
                item = gathered[index, number, 0:HEAD_DIM, :].astype(jnp.float32)
                state = state * (tail[0:1, :] + tail[1:2, :]) + item
            chain_out[number] = state.astype(jnp.bfloat16)

            @pl.when(hi + 1 < hi_size)
            def _():
                chain_copy(number).start()

            for index in range(members):

                @pl.when(member != index)
                def _():
                    deliver_copy(index, number).start()

            carried[member * own_heads + number] = deliver_out[member * own_heads + number]
            return carry

        lax.fori_loop(0, own_heads, body, 0)

    def take_states():
        def body(head, carry):
            @pl.when(head // own_heads != member)
            def _():
                deliver_arrival(head).wait_recv()

            return carry

        lax.fori_loop(0, heads, body, 0)

    gain = gain_ref[...]

    def local_body(head, carry):
        causal = lower_triangle()
        lanes = lanes_of(head)
        middle = SPAN // 2
        for span in range(spans):
            part = span_rows(span)
            running = running_ref[part, lanes]
            anchor = running[middle - 1 : middle, :]
            queries = silu(query_ref[part, lanes].astype(jnp.float32)) * (HEAD_DIM**-0.5)
            reach = queries * jnp.exp(running - anchor)
            back = keys_ref[part, lanes] * jnp.exp(anchor - running)
            scores = dot(reach.astype(jnp.bfloat16), back.astype(jnp.bfloat16), NT)
            scores = jnp.where(causal, scores, 0.0).astype(jnp.bfloat16)
            out = dot(scores, value_ref[part, lanes])
            if span > 0:
                out = out + dot(
                    (reach * jnp.exp(anchor)).astype(jnp.bfloat16), starts_ref[head, span - 1], NT
                )
            local_ref[part, lanes] = out
            base = base_ref[head, span : span + 1, :]
            reach_ref[part, lanes] = (reach * jnp.exp(anchor + base)).astype(jnp.bfloat16)
            gated_ref[part, lanes] = gain * silu(gate_ref[part, lanes].astype(jnp.float32))
        return carry

    def keeps(index, group):
        return (index * groups + group) % 2 == lo

    def group_lanes(index, group, which):
        start = which * half_width + (index * groups + group) // 2 * per * HEAD_DIM
        return pl.ds(pl.multiple_of(start, HEAD_DIM), per * HEAD_DIM)

    def swap_copy(group, span):
        start = 2 * half_width + group * per * HEAD_DIM
        return remote(
            mixed_ref.at[span_rows(span), pl.ds(start, per * HEAD_DIM)],
            mixed_ref.at[span_rows(span), group_lanes(tp, group, 1)],
            swap_send.at[group // 2],
            swap_recv.at[group // 2, span],
            {"lo": 1 - lo},
        )

    def origin_of(index, mask):
        for bit, by in enumerate(strides):
            if (mask >> bit) & 1:
                index = flipped(index, by)
        return index

    def tp_copy(stage, which, mask, group, span):
        block = mixed_ref.at[span_rows(span), group_lanes(origin_of(tp, mask), group, which)]
        return remote(
            block,
            block,
            tp_send.at[(1 << stage) - 1 + mask, which, group // 2],
            tp_recv.at[(1 << stage) - 1 + mask, which, group // 2, span],
            {"tp": flipped(tp, strides[stage])},
        )

    def mix(span):
        part = span_rows(span)
        for head in range(heads):
            lanes = lanes_of(head)
            out = local_ref[part, lanes] + dot(reach_ref[part, lanes], carried[head], NT)
            mean_sq = jnp.mean(out * out, axis=1, keepdims=True)
            mixed = out * lax.rsqrt(mean_sq + EPSILON) * gated_ref[part, lanes]
            group = head // per
            kept_start = (tp * groups + group) // 2 * per * HEAD_DIM + head % per * HEAD_DIM
            away_start = 2 * half_width + head * HEAD_DIM
            start = jnp.where(keeps(tp, group), kept_start, away_start)
            mixed_ref[part, pl.ds(pl.multiple_of(start, HEAD_DIM), HEAD_DIM)] = mixed.astype(
                jnp.bfloat16
            )

    def send_away(span):
        for group in range(groups):

            @pl.when(jnp.logical_not(keeps(tp, group)))
            def _():
                swap_copy(group, span).start()

    def send_kept(span):
        for group in range(groups):

            @pl.when(keeps(tp, group))
            def _():
                for stage in range(len(strides)):
                    tp_copy(stage, 0, 0, group, span).start()

    def take_swap(span):
        for group in range(groups):

            @pl.when(keeps(tp, group))
            def _():
                swap_copy(group, span).wait_recv()
                for stage in range(len(strides)):
                    tp_copy(stage, 1, 0, group, span).start()

    def take_stage(stage, which, span):
        peer = flipped(tp, strides[stage])
        for mask in range(1 << stage):
            for group in range(groups):

                @pl.when(keeps(origin_of(peer, mask), group))
                def _():
                    tp_copy(stage, which, mask, group, span).wait_recv()
                    for later in range(stage + 1, len(strides)):
                        tp_copy(later, which, mask | (1 << stage), group, span).start()

    def partial_copy(piece, span):
        return remote(
            partial_out.at[piece, span],
            partial_in.at[piece, span],
            partial_send.at[0],
            partial_recv.at[piece, span],
            {"lo": 1 - lo},
        )

    def both(span, start, depth):
        part = span_rows(span)
        start = pl.multiple_of(start, HEAD_DIM)
        later = pl.multiple_of(start + half_width, HEAD_DIM)
        return jnp.concatenate(
            [mixed_ref[part, pl.ds(later, depth)], mixed_ref[part, pl.ds(start, depth)]], axis=0
        )

    def multiply_near(span):
        start = near_block * block_depth
        left = both(span, start, near)
        rows_near = pl.ds(pl.multiple_of(start, HEAD_DIM), near)
        for number in range(tiles):
            lanes = pl.ds(number * tile, tile)
            total_ref[span, :, lanes] = dot(left, whole_weight[rows_near, lanes])

    def multiply_away(piece):
        start = away_block * block_depth
        rows_away = pl.ds(pl.multiple_of(start, HEAD_DIM), away)
        lanes = pl.ds(piece * weight_tile, weight_tile)
        right = whole_weight[rows_away, lanes]
        for span in range(spans):
            total = total_ref[span, :, lanes] + dot(both(span, start, away), right)
            partial_out[piece, span] = total[0:SPAN].astype(jnp.bfloat16)
            partial_copy(piece, span).start()
            total_ref[span, SPAN:, lanes] = total[SPAN:]

    def square_copy(step):
        return remote(
            squares_ref.at[tp],
            squares_ref.at[tp],
            square_send.at[step - 1],
            square_recv.at[step - 1],
            {"tp": (tp + step) % tp_size},
        )

    def combine(piece, span):
        lanes = pl.ds(piece * weight_tile, weight_tile)
        partial_copy(piece, span).wait_recv()
        total = total_ref[span, SPAN:, lanes] + partial_in[piece, span].astype(jnp.float32)
        rounded = total.astype(jnp.bfloat16)
        projected_ref[span_rows(span), lanes] = rounded
        branch = rounded.astype(jnp.float32)
        branch = branch * branch
        squares = branch[:, 0:HEAD_DIM]
        for start in range(HEAD_DIM, weight_tile, HEAD_DIM):
            squares = squares + branch[:, start : start + HEAD_DIM]
        if piece > 0:
            squares = squares + sums_ref[span]
        sums_ref[span] = squares

    def total_squares(span):
        column = jnp.sum(sums_ref[span], axis=1, keepdims=True)
        row = jnp.sum(jnp.where(diagonal(), column, 0.0), axis=0, keepdims=True)
        squares_ref[tp, span : span + 1, :] = row

    def finish():
        for step in range(1, tp_size):
            square_copy(step).wait_recv()
        total = squares_ref[0, 0:spans, :]
        for index in range(1, tp_size):
            total = total + squares_ref[index, 0:spans, :]
        scale_ref[...] = lax.rsqrt(total * (1.0 / (columns * tp_size)) + EPSILON)

    def lines_sent(first, last):
        for hop in range(first, last):
            for way in (0, 1):

                @pl.when(sends(way, hop))
                def _():
                    line_sent(way, hop).wait_send()

    def states_sent():
        others = (members - 1) * own_heads
        next_member = member_at((member + 1) % members)
        pltpu.make_async_remote_copy(
            src_ref=state_out.at[pl.ds(0, others)],
            dst_ref=state_out.at[pl.ds(0, others)],
            send_sem=gather_send.at[0],
            recv_sem=gather_recv.at[0, 0],
            device_id=next_member,
            device_id_type=MESH_ID,
        ).wait_send()
        pltpu.make_async_remote_copy(
            src_ref=deliver_out.at[pl.ds(0, others)],
            dst_ref=deliver_out.at[pl.ds(0, others)],
            send_sem=deliver_send.at[0],
            recv_sem=deliver_recv.at[0],
            device_id=next_member,
            device_id_type=MESH_ID,
        ).wait_send()

        @pl.when(hi + 1 < hi_size)
        def _():
            remote(
                chain_out, chain_in, chain_send.at[0], chain_recv.at[0], {"hi": hi + 1}
            ).wait_send()

    def mixed_sent():
        for group in range(groups):
            block = mixed_ref.at[:, group_lanes(tp, group, 0)]

            @pl.when(jnp.logical_not(keeps(tp, group)))
            def _():
                remote(
                    block, block, swap_send.at[group // 2], swap_recv.at[0, 0], {"lo": 1 - lo}
                ).wait_send()

            for stage in range(len(strides)):
                for which in (0, 1):
                    for mask in range(1 << stage):

                        @pl.when(keeps(origin_of(tp, mask), group))
                        def _():
                            remote(
                                block,
                                block,
                                tp_send.at[(1 << stage) - 1 + mask, which, group // 2],
                                tp_recv.at[0, 0, 0, 0],
                                {"tp": flipped(tp, strides[stage])},
                            ).wait_send()

    early = hi < hi_size // 2
    scope = jax.named_scope

    def local():
        with scope("local"):
            lax.fori_loop(0, heads, local_body, 0)

    def hop_pieces(hop, way, first, last):
        with scope(f"hop{hop}_{way}_{first}"):
            for piece in range(first, last):
                take_hop(hop, way, piece)

    loads[0].wait()
    for piece in range(pieces):
        if piece < 3:
            start_line(0, piece)
        elif piece < 7:

            @pl.when(hi == hi_size - 2)
            def _():
                start_line(0, piece)

        start_line(1, piece)
    for piece in range(pieces):
        start_side(piece)
    loads[1].wait()
    loads[2].wait()
    with scope("state"):
        lax.fori_loop(0, heads, state_body, 0)
    loads[3].wait()
    loads[4].wait()

    @pl.when(jnp.logical_not(early))
    def _():
        local()

    with scope("chain"):
        chain_states()
    for piece in range(3, pieces):
        if piece < 7:

            @pl.when(hi != hi_size - 2)
            def _():
                start_line(0, piece)

        else:
            start_line(0, piece)

    @pl.when(early)
    def _():
        local()

    with scope("take_states"):
        take_states()
    with scope("mix"):
        for span in range(spans):
            mix(span)
            send_away(span)
            if span < 2:
                send_kept(span)
    hop_pieces(1, 1, 0, 6)
    hop_pieces(1, 0, 0, 3)
    with scope("swap01"):
        for span in range(2):
            take_swap(span)
            send_kept(span + 2)
    hop_pieces(1, 1, 6, 8)
    hop_pieces(1, 0, 3, 4)

    def take_rest(span):
        with scope(f"take{span}"):
            for stage in range(1, len(strides)):
                for which in (0, 1):
                    take_stage(stage, which, span)

    with scope("y0"):
        take_stage(0, 0, 0)
        take_swap(2)
        take_stage(0, 0, 1)
        take_stage(0, 1, 0)
    hop_pieces(1, 0, 4, 8)
    hop_pieces(2, 1, 0, 3)
    def near_part(span):
        if hi_size <= 4:
            take_rest(span)
            if span == 0:
                take_near_sides()
            with scope(f"near{span}"):
                multiply_near(span)

    near_part(0)
    with scope("y1"):
        take_swap(3)
        take_stage(0, 0, 2)
        take_stage(0, 1, 1)
        take_stage(0, 0, 3)
    hop_pieces(2, 1, 3, 5)
    hop_pieces(2, 0, 0, 3)
    near_part(1)
    with scope("y2"):
        take_stage(0, 1, 2)
        take_stage(0, 1, 3)
    near_part(2)
    near_part(3)
    hop_pieces(2, 1, 5, 8)
    hop_pieces(2, 0, 3, 8)
    if hi_size > 4:
        for hop in range(3, hi_size - 1):
            for way in (0, 1):
                hop_pieces(hop, way, 0, pieces)
        take_near_sides()
        for span in range(spans):
            take_rest(span)
            multiply_near(span)
    for piece in range(pieces):
        with scope(f"far_wait{piece}"):
            if hi_size > 3:
                for way in (0, 1):
                    take_hop(hi_size - 1, way, piece)
            take_away_sides(piece)
        with scope(f"far{piece}"):
            multiply_away(piece)
        with scope(f"sent{piece}"):
            if piece == 0:
                states_sent()
            if piece == 1:
                mixed_sent()
            if piece == pieces - 3:
                lines_sent(1, 2)
            if piece == pieces - 2:
                lines_sent(2, min(3, hi_size))
            if piece == pieces - 1:
                lines_sent(3, hi_size)
        if piece > 0:
            with scope(f"combine{piece - 1}"):
                for span in range(spans):
                    combine(piece - 1, span)
    with scope("combine_last"):
        for span in range(spans):
            combine(pieces - 1, span)
        for span in range(spans):
            total_squares(span)
        for step in range(1, tp_size):
            square_copy(step).start()
    with scope("drain"):
        for piece in range(pieces):
            for reach in range(1, inner_size):
                for block_hi in range(hi_size):
                    side_copy(reach, block_hi, piece).wait_send()
        remote(
            partial_out, partial_in, partial_send.at[0], partial_recv.at[0, 0], {"lo": 1 - lo}
        ).wait_send()
    with scope("finish"):
        finish()
        for step in range(1, tp_size):
            square_copy(step).wait_send()


def layer(sizes, arrays):
    hi_size, inner_size, tp_size, per, tile, weight_tile = sizes
    rows, width = arrays[0].shape
    depth, columns = arrays[7].shape
    heads = width // HEAD_DIM
    groups = heads // per
    spans = rows // SPAN
    members = 2 * inner_size
    own_heads = heads // members
    kept = (groups + 1) // 2
    half_width = heads * tp_size // 2 * HEAD_DIM
    pieces = columns // weight_tile
    vmem = pl.BlockSpec(memory_space=pltpu.VMEM)
    anywhere = pl.BlockSpec(memory_space=pl.ANY)
    item = (HEAD_DIM + TAIL, HEAD_DIM)
    square = (HEAD_DIM, HEAD_DIM)
    bf16, f32 = jnp.bfloat16, jnp.float32
    dma = pltpu.SemaphoreType.DMA
    return pl.pallas_call(
        functools.partial(layer_kernel, sizes),
        in_specs=[anywhere] * 4 + [vmem] * 3 + [anywhere],
        out_specs=[vmem, vmem],
        out_shape=[
            pltpu.VMEM((rows, columns), bf16),
            pltpu.VMEM((spans, HEAD_DIM), f32),
        ],
        scratch_shapes=[
            pltpu.VMEM((hi_size * inner_size * depth, columns), bf16),
            pltpu.VMEM((rows, width), bf16),
            pltpu.VMEM((rows, width), bf16),
            pltpu.VMEM((rows, width), bf16),
            pltpu.VMEM((rows, width), bf16),
            pltpu.VMEM((rows, width), f32),
            pltpu.VMEM((rows, width), f32),
            pltpu.VMEM((heads, max(8, spans), HEAD_DIM), f32),
            pltpu.VMEM((heads, max(1, spans - 1)) + square, bf16),
            pltpu.VMEM((heads,) + item, bf16),
            pltpu.VMEM((members, own_heads) + item, bf16),
            pltpu.VMEM((own_heads,) + square, bf16),
            pltpu.VMEM((own_heads,) + square, bf16),
            pltpu.VMEM((heads,) + square, bf16),
            pltpu.VMEM((heads,) + square, bf16),
            pltpu.VMEM((rows, width), f32),
            pltpu.VMEM((rows, width), bf16),
            pltpu.VMEM((rows, width), f32),
            pltpu.VMEM((rows, 2 * half_width + width), bf16),
            pltpu.VMEM((pieces, spans, SPAN, weight_tile), bf16),
            pltpu.VMEM((pieces, spans, SPAN, weight_tile), bf16),
            pltpu.VMEM((spans, 2 * SPAN, columns), f32),
            pltpu.VMEM((spans, SPAN, HEAD_DIM), f32),
            pltpu.VMEM((tp_size, max(8, spans), HEAD_DIM), f32),
            dma((5,)),
            dma((1,)),
            dma((members, own_heads)),
            dma((1,)),
            dma((own_heads,)),
            dma((1,)),
            dma((heads,)),
            dma((kept,)),
            dma((kept, spans)),
            dma((tp_size - 1, 2, kept)),
            dma((tp_size - 1, 2, kept, spans)),
            dma((2, max(1, hi_size - 1))),
            dma((hi_size, pieces)),
            dma((2, inner_size - 1, hi_size, pieces) if inner_size > 1 else (1,)),
            dma((1,)),
            dma((pieces, spans)),
            dma((tp_size - 1,)),
            dma((tp_size - 1,)),
        ],
        name="layer",
        compiler_params=pltpu.CompilerParams(
            collective_id=0, has_side_effects=True, vmem_limit_bytes=62800 * 1024
        ),
        cost_estimate=pl.CostEstimate(
            flops=rows * width * 10000, bytes_accessed=14 * rows * width, transcendentals=0
        ),
    )(*arrays)


def per_device(hi_size, inner_size, tp_size, *arrays):
    query, forget, value, gate, gap, surge, head_gain, matrix, branch_gain, residual = arrays
    per = inner_size * matrix.shape[0] // HEAD_DIM
    projected, scale = layer(
        (hi_size, inner_size, tp_size, per, 256, 128),
        (
            query,
            forget,
            value,
            gate,
            gap.reshape(-1, HEAD_DIM),
            surge,
            head_gain.reshape(1, HEAD_DIM),
            matrix,
        ),
    )
    columns = matrix.shape[1]
    gain_part = lax.dynamic_slice_in_dim(branch_gain, lax.axis_index("tp") * columns, columns)
    branch = projected.astype(jnp.float32) * scale.reshape(-1)[:, None] * gain_part
    return (residual.astype(jnp.float32) + branch).astype(jnp.bfloat16)


def solution(mesh):
    sp_size, tp_size = mesh.shape["sp"], mesh.shape["tp"]
    sp = ("hi", "lo", "inner")
    placed = (
        P(sp, "tp"),
        P(sp, "tp"),
        P(sp, "tp"),
        P(sp, "tp"),
        P(),
        P("tp", sp),
        P(),
        P(sp, "tp"),
        P(),
        P(sp, "tp"),
    )

    def whole(*arrays):
        inner = max(1, HEAD_DIM * sp_size // arrays[7].shape[0])
        hi = sp_size // (2 * inner)
        devices = mesh.devices.reshape(hi, 2, inner, tp_size)
        paired = Mesh(devices, ("hi", "lo", "inner", "tp"))
        return jax.shard_map(
            functools.partial(per_device, hi, inner, tp_size),
            mesh=paired,
            in_specs=placed,
            out_specs=P(sp, "tp"),
            check_vma=False,
        )(*arrays)

    return whole
```

```python
import functools

import jax
import jax.numpy as jnp
from jax import lax
from jax.experimental import pallas as pl
from jax.experimental.pallas import tpu as pltpu
from jax.sharding import Mesh
from jax.sharding import PartitionSpec as P

HEAD_DIM = 128
SPAN = 128
TAIL = 16
EPSILON = 1e-06
NT = (((1,), (1,)), ((), ()))
TN = (((0,), (0,)), ((), ()))
NN = (((1,), (0,)), ((), ()))
MESH_ID = pl.DeviceIdType.MESH


def dot(a, b, dims=NN):
    return lax.dot_general(a, b, dims, preferred_element_type=jnp.float32)


def lower_triangle():
    rows = lax.broadcasted_iota(jnp.int32, (SPAN, SPAN), 0)
    columns = lax.broadcasted_iota(jnp.int32, (SPAN, SPAN), 1)
    return rows >= columns


def diagonal():
    rows = lax.broadcasted_iota(jnp.int32, (SPAN, SPAN), 0)
    columns = lax.broadcasted_iota(jnp.int32, (SPAN, SPAN), 1)
    return rows == columns


def silu(logits):
    return logits / (1.0 + jnp.exp(-logits))


def decays(logits, gap, surge, causal):
    keys = gap / (1.0 + jnp.exp(logits.astype(jnp.float32)))
    series = keys * (1.0 / 7.0) + (1.0 / 6.0)
    for order in (5, 4, 3, 2):
        series = series * keys + (1.0 / order)
    logs = -(series * keys + 1.0) * keys
    high = logs.astype(jnp.bfloat16)
    low = (logs - high.astype(jnp.float32)).astype(jnp.bfloat16)
    ones = causal.astype(jnp.bfloat16)
    surged = jnp.sum(jnp.where(causal, surge, 0.0), axis=1, keepdims=True)
    return keys, dot(ones, high) + dot(ones, low) + surged


def layer_kernel(
    sizes,
    query_in,
    forget_in,
    value_in,
    gate_in,
    gap_ref,
    surge_ref,
    gain_ref,
    weight_in,
    projected_ref,
    scale_ref,
    whole_weight,
    relay,
    query_ref,
    forget_ref,
    value_ref,
    gate_ref,
    running_ref,
    keys_ref,
    base_ref,
    starts_ref,
    state_out,
    gathered,
    chain_in,
    chain_out,
    deliver_out,
    carried,
    local_ref,
    reach_ref,
    gated_ref,
    mixed_ref,
    partial_out,
    partial_in,
    total_ref,
    sums_ref,
    squares_ref,
    load_sems,
    gather_send,
    gather_recv,
    chain_send,
    chain_recv,
    deliver_send,
    deliver_recv,
    swap_send,
    swap_recv,
    tp_send,
    tp_recv,
    line_send,
    line_recv,
    side_send,
    side_recv,
    partial_send,
    partial_recv,
    square_send,
    square_recv,
):
    hi_size, inner_size, tp_size, per, tile, weight_tile = sizes
    rows, width = query_in.shape
    depth, columns = weight_in.shape
    heads = width // HEAD_DIM
    spans = rows // SPAN
    groups = heads // per
    half_width = heads * tp_size // 2 * HEAD_DIM
    members = inner_size
    lines = 2 * hi_size
    own_heads = heads // members
    tiles = columns // tile
    pieces = columns // weight_tile
    hi, lo, inner, tp = (lax.axis_index(a) for a in ("hi", "lo", "inner", "tp"))
    member = inner
    line = hi * 2 + lo
    strides = []
    by = tp_size // 2
    while by >= 1:
        strides.append(by)
        by //= 2

    def member_at(index):
        return {"inner": index}

    def on_line(index):
        return {"hi": index // 2, "lo": index % 2}

    def flipped(index, by):
        return index + by - 2 * by * ((index // by) % 2)

    def remote(source, target, send, recv, device):
        return pltpu.make_async_remote_copy(
            src_ref=source,
            dst_ref=target,
            send_sem=send,
            recv_sem=recv,
            device_id=device,
            device_id_type=MESH_ID,
        )

    def span_rows(span):
        return pl.ds(span * SPAN, SPAN)

    def lanes_of(head):
        return pl.ds(pl.multiple_of(head * HEAD_DIM, HEAD_DIM), HEAD_DIM)

    def slot_rows(block_hi, block_inner):
        return pl.ds(pl.multiple_of((block_hi * inner_size + block_inner) * depth, depth), depth)

    loads = [
        pltpu.make_async_copy(source, target, load_sems.at[number])
        for number, (source, target) in enumerate(
            (
                (weight_in, whole_weight.at[slot_rows(hi, inner)]),
                (forget_in, forget_ref),
                (value_in, value_ref),
                (query_in, query_ref),
                (gate_in, gate_ref),
            )
        )
    ]
    for load in loads:
        load.start()

    barrier = pltpu.get_barrier_semaphore()

    peers = members - 1 + tp_size - 1
    for step in range(1, members):
        pl.semaphore_signal(
            barrier,
            inc=1,
            device_id=member_at((member + step) % members),
            device_id_type=MESH_ID,
        )
    for step in range(1, tp_size):
        pl.semaphore_signal(
            barrier, inc=1, device_id={"tp": (tp + step) % tp_size}, device_id_type=MESH_ID
        )
    for step in (1, -1):
        there = line + step
        inside = (there >= 0) & (there < lines)

        @pl.when(inside)
        def _():
            pl.semaphore_signal(barrier, inc=1, device_id=on_line(there), device_id_type=MESH_ID)

        peers = peers + jnp.where(inside, 1, 0)
    pl.semaphore_wait(barrier, peers)

    def piece_lanes(piece):
        return pl.ds(piece * weight_tile, weight_tile)

    def weight_block(block_hi, block_inner, piece):
        return whole_weight.at[slot_rows(block_hi, block_inner), piece_lanes(piece)]

    def step_of(way):
        return 1 if way == 0 else -1

    def line_block(origin, distance, piece):
        block_hi = origin // 2
        if distance % 2 == 0:
            return weight_block(block_hi, inner, piece)
        return relay.at[
            pl.ds(pl.multiple_of(block_hi * depth, depth), depth), piece_lanes(piece)
        ]

    def line_copy(way, hop, piece):
        origin = line - step_of(way) * (hop - 1)
        return remote(
            line_block(origin, hop - 1, piece),
            line_block(origin, hop, piece),
            line_send.at[way, hop - 1],
            line_recv.at[origin, piece],
            on_line(line + step_of(way)),
        )

    def line_arrival(origin, piece):
        block = weight_block(hi, inner, piece)
        return remote(
            block, block, line_send.at[0, 0], line_recv.at[origin, piece], on_line(origin)
        )

    def line_sent(way, hop):
        block = whole_weight.at[slot_rows(hi, inner)]
        return remote(
            block,
            block,
            line_send.at[way, hop - 1],
            line_recv.at[0, 0],
            on_line(line + step_of(way)),
        )

    def inside(index):
        return (index >= 0) & (index < lines)

    def sends(way, hop):
        step = step_of(way)
        last = line + step * (1 + hop % 2)
        return inside(line - step * (hop - 1)) & inside(last)

    def receives(way, hop):
        step = step_of(way)
        return inside(line - step * hop) & inside(line + step * (hop % 2))

    def side_copy(reach, block_hi, piece):
        block = weight_block(block_hi, inner, piece)
        return remote(
            block,
            block,
            side_send.at[reach - 1],
            side_recv.at[reach - 1, block_hi, piece],
            {"inner": (inner + reach) % inner_size},
        )

    def start_line(way, piece):
        @pl.when(sends(way, 1))
        def _():
            line_copy(way, 1, piece).start()

    def start_side(piece):
        for reach in range(1, inner_size):
            side_copy(reach, hi, piece).start()

    def take_hop(hop, way, piece):
        if hop >= lines:
            return
        origin = line - step_of(way) * hop

        @pl.when(receives(way, hop))
        def _():
            line_arrival(origin, piece).wait_recv()
            if hop % 2 == 0:
                for reach in range(1, inner_size):
                    side_copy(reach, origin // 2, piece).start()

        if hop + 1 < lines:

            @pl.when(sends(way, hop + 1))
            def _():
                line_copy(way, hop + 1, piece).start()

    def take_sides(piece):
        for reach in range(1, inner_size):
            for block_hi in range(hi_size):
                side_copy(reach, block_hi, piece).wait_recv()

    def sides_sent():
        for reach in range(1, inner_size):
            remote(
                whole_weight.at[pl.ds(0, hi_size * depth)],
                whole_weight.at[pl.ds(0, hi_size * depth)],
                side_send.at[reach - 1],
                side_recv.at[0, 0, 0],
                {"inner": (inner + reach) % inner_size},
            ).wait_send()

    def state_copy(head):
        return remote(
            state_out.at[head],
            gathered.at[member, head % own_heads],
            gather_send.at[0],
            gather_recv.at[member, head % own_heads],
            member_at(head // own_heads),
        )

    def state_arrival(index, number):
        return remote(
            state_out.at[0],
            gathered.at[index, number],
            gather_send.at[0],
            gather_recv.at[index, number],
            member_at(index),
        )

    def chain_copy(number):
        return remote(
            chain_out.at[number],
            chain_in.at[number],
            chain_send.at[0],
            chain_recv.at[number],
            on_line(line + 1),
        )

    def deliver_copy(index, number):
        head = member * own_heads + number
        return remote(
            deliver_out.at[index * own_heads + number],
            carried.at[head],
            deliver_send.at[0],
            deliver_recv.at[head],
            member_at(index),
        )

    def deliver_arrival(head):
        return remote(
            deliver_out.at[0],
            carried.at[head],
            deliver_send.at[0],
            deliver_recv.at[head],
            member_at(head // own_heads),
        )

    def state_body(turn, carry):
        head = (turn + (member + 1) * own_heads) % heads
        causal = lower_triangle()
        gap = gap_ref[pl.ds(tp * heads + head, 1), :]
        lanes = lanes_of(head)
        this_head = lax.broadcasted_iota(jnp.int32, (heads, SPAN), 0) == head
        state = jnp.zeros((HEAD_DIM, HEAD_DIM), jnp.float32)
        base = jnp.zeros((1, HEAD_DIM), jnp.float32)
        for span in range(spans):
            part = span_rows(span)
            surge = jnp.sum(jnp.where(this_head, surge_ref[:, part], 0.0), axis=0, keepdims=True)
            keys, running = decays(forget_ref[part, lanes], gap, surge, causal)
            keys_ref[part, lanes] = keys
            running_ref[part, lanes] = running
            base_ref[head, span : span + 1, :] = base
            if span > 0:
                starts_ref[head, span - 1] = state.astype(jnp.bfloat16)
            ending = running[SPAN - 1 : SPAN, :]
            kept = (keys * jnp.exp(ending - running)).astype(jnp.bfloat16)
            state = state * jnp.exp(ending) + dot(value_ref[part, lanes], kept, TN)
            base = base + ending
        decay = jnp.exp(base)
        high = decay.astype(jnp.bfloat16).astype(jnp.float32)
        first = lax.broadcasted_iota(jnp.int32, (TAIL, HEAD_DIM), 0) == 0
        item = state.astype(jnp.bfloat16)
        tail = jnp.where(first, high, decay - high).astype(jnp.bfloat16)
        state_out[head, 0:HEAD_DIM, :] = item
        state_out[head, HEAD_DIM:, :] = tail
        owner = head // own_heads

        @pl.when(owner == member)
        def _():
            gathered[member, head % own_heads, 0:HEAD_DIM, :] = item
            gathered[member, head % own_heads, HEAD_DIM:, :] = tail

        @pl.when(owner != member)
        def _():
            state_copy(head).start()

        return carry

    def chain_states():
        @pl.when(line == 0)
        def _():
            chain_in[...] = jnp.zeros_like(chain_in)

        def body(number, carry):
            for index in range(members):

                @pl.when(member != index)
                def _():
                    state_arrival(index, number).wait_recv()

            @pl.when(line > 0)
            def _():
                chain_copy(number).wait_recv()

            state = chain_in[number].astype(jnp.float32)
            for index in range(members):
                deliver_out[index * own_heads + number] = state.astype(jnp.bfloat16)
                tail = gathered[index, number, HEAD_DIM:, :].astype(jnp.float32)
                item = gathered[index, number, 0:HEAD_DIM, :].astype(jnp.float32)
                state = state * (tail[0:1, :] + tail[1:2, :]) + item
            chain_out[number] = state.astype(jnp.bfloat16)

            @pl.when(line + 1 < lines)
            def _():
                chain_copy(number).start()

            for index in range(members):

                @pl.when(member != index)
                def _():
                    deliver_copy(index, number).start()

            carried[member * own_heads + number] = deliver_out[member * own_heads + number]
            return carry

        lax.fori_loop(0, own_heads, body, 0)

    def take_states():
        def body(head, carry):
            @pl.when(head // own_heads != member)
            def _():
                deliver_arrival(head).wait_recv()

            return carry

        lax.fori_loop(0, heads, body, 0)

    gain = gain_ref[...]

    def local_body(head, carry):
        causal = lower_triangle()
        lanes = lanes_of(head)
        middle = SPAN // 2
        for span in range(spans):
            part = span_rows(span)
            running = running_ref[part, lanes]
            anchor = running[middle - 1 : middle, :]
            queries = silu(query_ref[part, lanes].astype(jnp.float32)) * (HEAD_DIM**-0.5)
            reach = queries * jnp.exp(running - anchor)
            back = keys_ref[part, lanes] * jnp.exp(anchor - running)
            scores = dot(reach.astype(jnp.bfloat16), back.astype(jnp.bfloat16), NT)
            scores = jnp.where(causal, scores, 0.0).astype(jnp.bfloat16)
            out = dot(scores, value_ref[part, lanes])
            if span > 0:
                out = out + dot(
                    (reach * jnp.exp(anchor)).astype(jnp.bfloat16), starts_ref[head, span - 1], NT
                )
            local_ref[part, lanes] = out
            base = base_ref[head, span : span + 1, :]
            reach_ref[part, lanes] = (reach * jnp.exp(anchor + base)).astype(jnp.bfloat16)
            gated_ref[part, lanes] = gain * silu(gate_ref[part, lanes].astype(jnp.float32))
        return carry

    def keeps(index, group):
        return (index * groups + group) % 2 == lo

    def group_lanes(index, group, which):
        start = which * half_width + (index * groups + group) // 2 * per * HEAD_DIM
        return pl.ds(pl.multiple_of(start, HEAD_DIM), per * HEAD_DIM)

    def swap_copy(group, span):
        start = 2 * half_width + group * per * HEAD_DIM
        return remote(
            mixed_ref.at[span_rows(span), pl.ds(start, per * HEAD_DIM)],
            mixed_ref.at[span_rows(span), group_lanes(tp, group, 1)],
            swap_send.at[group // 2],
            swap_recv.at[group // 2, span],
            {"lo": 1 - lo},
        )

    def origin_of(index, mask):
        for bit, by in enumerate(strides):
            if (mask >> bit) & 1:
                index = flipped(index, by)
        return index

    def tp_copy(stage, which, mask, group, span):
        block = mixed_ref.at[span_rows(span), group_lanes(origin_of(tp, mask), group, which)]
        return remote(
            block,
            block,
            tp_send.at[(1 << stage) - 1 + mask, which, group // 2],
            tp_recv.at[(1 << stage) - 1 + mask, which, group // 2, span],
            {"tp": flipped(tp, strides[stage])},
        )

    def mix(span):
        part = span_rows(span)
        for head in range(heads):
            lanes = lanes_of(head)
            out = local_ref[part, lanes] + dot(reach_ref[part, lanes], carried[head], NT)
            mean_sq = jnp.mean(out * out, axis=1, keepdims=True)
            mixed = out * lax.rsqrt(mean_sq + EPSILON) * gated_ref[part, lanes]
            group = head // per
            kept_start = (tp * groups + group) // 2 * per * HEAD_DIM + head % per * HEAD_DIM
            away_start = 2 * half_width + head * HEAD_DIM
            start = jnp.where(keeps(tp, group), kept_start, away_start)
            mixed_ref[part, pl.ds(pl.multiple_of(start, HEAD_DIM), HEAD_DIM)] = mixed.astype(
                jnp.bfloat16
            )

    def send_away(span):
        for group in range(groups):

            @pl.when(jnp.logical_not(keeps(tp, group)))
            def _():
                swap_copy(group, span).start()

    def send_kept(span):
        for group in range(groups):

            @pl.when(keeps(tp, group))
            def _():
                for stage in range(len(strides)):
                    tp_copy(stage, 0, 0, group, span).start()

    def take_swap(span):
        for group in range(groups):

            @pl.when(keeps(tp, group))
            def _():
                swap_copy(group, span).wait_recv()
                for stage in range(len(strides)):
                    tp_copy(stage, 1, 0, group, span).start()

    def take_stage(stage, which, span):
        peer = flipped(tp, strides[stage])
        for mask in range(1 << stage):
            for group in range(groups):

                @pl.when(keeps(origin_of(peer, mask), group))
                def _():
                    tp_copy(stage, which, mask, group, span).wait_recv()
                    for later in range(stage + 1, len(strides)):
                        tp_copy(later, which, mask | (1 << stage), group, span).start()

    def partial_copy(piece, span):
        return remote(
            partial_out.at[piece, span],
            partial_in.at[piece, span],
            partial_send.at[0],
            partial_recv.at[piece, span],
            {"lo": 1 - lo},
        )

    def both(span, start, depth):
        part = span_rows(span)
        return jnp.concatenate(
            [mixed_ref[part, half_width : 2 * half_width], mixed_ref[part, 0:half_width]], axis=0
        )

    def multiply(piece, part):
        lanes = piece_lanes(piece)
        right = whole_weight[:, lanes]
        for span in part:
            total = dot(both(span, 0, half_width), right)
            partial_out[piece, span] = total[0:SPAN].astype(jnp.bfloat16)
            partial_copy(piece, span).start()
            total_ref[span, :, lanes] = total[SPAN:]

    def square_copy(step):
        return remote(
            squares_ref.at[tp],
            squares_ref.at[tp],
            square_send.at[step - 1],
            square_recv.at[step - 1],
            {"tp": (tp + step) % tp_size},
        )

    def combine(piece, span):
        lanes = pl.ds(piece * weight_tile, weight_tile)
        partial_copy(piece, span).wait_recv()
        total = total_ref[span, :, lanes] + partial_in[piece, span].astype(jnp.float32)
        rounded = total.astype(jnp.bfloat16)
        projected_ref[span_rows(span), lanes] = rounded
        branch = rounded.astype(jnp.float32)
        branch = branch * branch
        squares = branch[:, 0:HEAD_DIM]
        for start in range(HEAD_DIM, weight_tile, HEAD_DIM):
            squares = squares + branch[:, start : start + HEAD_DIM]
        if piece > 0:
            squares = squares + sums_ref[span]
        sums_ref[span] = squares

    def total_squares(span):
        column = jnp.sum(sums_ref[span], axis=1, keepdims=True)
        row = jnp.sum(jnp.where(diagonal(), column, 0.0), axis=0, keepdims=True)
        squares_ref[tp, span : span + 1, :] = row

    def finish():
        for step in range(1, tp_size):
            square_copy(step).wait_recv()
        total = squares_ref[0, 0:spans, :]
        for index in range(1, tp_size):
            total = total + squares_ref[index, 0:spans, :]
        scale_ref[...] = lax.rsqrt(total * (1.0 / (columns * tp_size)) + EPSILON)

    def lines_sent(first, last):
        for hop in range(first, last):
            for way in (0, 1):

                @pl.when(sends(way, hop))
                def _():
                    line_sent(way, hop).wait_send()

    def states_sent():
        others = (members - 1) * own_heads
        next_member = member_at((member + 1) % members)
        pltpu.make_async_remote_copy(
            src_ref=state_out.at[pl.ds(0, others)],
            dst_ref=state_out.at[pl.ds(0, others)],
            send_sem=gather_send.at[0],
            recv_sem=gather_recv.at[0, 0],
            device_id=next_member,
            device_id_type=MESH_ID,
        ).wait_send()
        pltpu.make_async_remote_copy(
            src_ref=deliver_out.at[pl.ds(0, others)],
            dst_ref=deliver_out.at[pl.ds(0, others)],
            send_sem=deliver_send.at[0],
            recv_sem=deliver_recv.at[0],
            device_id=next_member,
            device_id_type=MESH_ID,
        ).wait_send()

        @pl.when(line + 1 < lines)
        def _():
            remote(
                chain_out, chain_in, chain_send.at[0], chain_recv.at[0], on_line(line + 1)
            ).wait_send()

    def mixed_sent():
        for group in range(groups):
            block = mixed_ref.at[:, group_lanes(tp, group, 0)]

            @pl.when(jnp.logical_not(keeps(tp, group)))
            def _():
                remote(
                    block, block, swap_send.at[group // 2], swap_recv.at[0, 0], {"lo": 1 - lo}
                ).wait_send()

            for stage in range(len(strides)):
                for which in (0, 1):
                    for mask in range(1 << stage):

                        @pl.when(keeps(origin_of(tp, mask), group))
                        def _():
                            remote(
                                block,
                                block,
                                tp_send.at[(1 << stage) - 1 + mask, which, group // 2],
                                tp_recv.at[0, 0, 0, 0],
                                {"tp": flipped(tp, strides[stage])},
                            ).wait_send()

    early = line < 2
    ends = (line == 0) | (line == lines - 1)
    between = jnp.logical_not(ends)
    scope = jax.named_scope

    def local():
        with scope("local"):
            lax.fori_loop(0, heads, local_body, 0)

    def hop_pieces(hop, way, first, last):
        with scope(f"hop{hop}_{way}_{first}"):
            for piece in range(first, last):
                take_hop(hop, way, piece)

    low = line < lines // 2

    def outward(first, last):
        @pl.when(low)
        def _():
            hop_pieces(1, 1, first, last)

        @pl.when(jnp.logical_not(low))
        def _():
            hop_pieces(1, 0, first, last)

    def inward(first, last):
        @pl.when(low)
        def _():
            hop_pieces(1, 0, first, last)

        @pl.when(jnp.logical_not(low))
        def _():
            hop_pieces(1, 1, first, last)

    def own_sides(first, last):
        for piece in range(first, last):
            start_side(piece)

    loads[0].wait()
    for piece in range(pieces):
        if piece < 3:
            start_line(0, piece)
        elif piece == 3:

            @pl.when(line > 0)
            def _():
                start_line(0, piece)

        start_line(1, piece)
    own_sides(0, 1)
    loads[1].wait()
    loads[2].wait()
    with scope("state"):
        lax.fori_loop(0, heads, state_body, 0)
    own_sides(1, 3)
    outward(0, 2)

    @pl.when(jnp.logical_not(low))
    def _():
        hop_pieces(1, 1, 0, 2)

    loads[3].wait()
    loads[4].wait()

    @pl.when(jnp.logical_not(early))
    def _():
        local()

    with scope("chain"):
        chain_states()

    @pl.when(line == 0)
    def _():
        for piece in range(3, 6):
            start_line(0, piece)

    @pl.when(line > 0)
    def _():
        for piece in range(4, pieces):
            start_line(0, piece)

    @pl.when(between)
    def _():
        own_sides(3, pieces)

    outward(2, 4)

    @pl.when(early)
    def _():
        local()

    def end_hops(first, last):
        @pl.when(ends)
        def _():
            hop_pieces(2, 1, first, last)
            hop_pieces(2, 0, first, last)

    def between_hops(first, last):
        @pl.when(between)
        def _():
            hop_pieces(2, 1, first, last)
            hop_pieces(2, 0, first, last)


    @pl.when(low)
    def _():
        hop_pieces(1, 0, 0, 2)

    inward(2, 4)
    with scope("take_states"):
        take_states()
    with scope("mix"):
        for span in range(spans):
            mix(span)
            send_away(span)
            if span < 2:
                send_kept(span)


    @pl.when(line == 0)
    def _():
        for piece in range(6, pieces):
            start_line(0, piece)

    @pl.when(ends)
    def _():
        own_sides(3, 5)

    end_hops(0, 2)
    with scope("swap01"):
        for span in range(2):
            take_swap(span)
            send_kept(span + 2)

    @pl.when(ends)
    def _():
        own_sides(5, pieces)

    @pl.when(jnp.logical_not(low))
    def _():
        hop_pieces(1, 1, 4, pieces)

    between_hops(0, 2)

    @pl.when(low)
    def _():
        hop_pieces(1, 0, 4, 6)

    def take_rest(span):
        with scope(f"take{span}"):
            for stage in range(1, len(strides)):
                for which in (0, 1):
                    take_stage(stage, which, span)

    with scope("y0"):
        take_stage(0, 0, 0)
        take_stage(0, 0, 1)
        take_swap(2)
        take_swap(3)
    outward(4, 6)
    with scope("y1"):
        take_stage(0, 1, 0)
        take_stage(0, 1, 1)
    take_rest(0)
    take_rest(1)
    outward(6, pieces)

    @pl.when(low)
    def _():
        hop_pieces(1, 0, 6, pieces)

    end_hops(2, 4)
    if lines > 4:
        between_hops(2, pieces)
        end_hops(4, pieces)
    for hop in range(3, lines):
        for way in (0, 1):
            hop_pieces(hop, way, 0, pieces)
    done = []
    order = []

    def advance(part, first, last):
        for piece in range(first, last):
            if not any(piece == other for other, _ in order):
                with scope(f"sides{piece}"):
                    take_sides(piece)
            with scope(f"mult{part[0]}_{piece}"):
                multiply(piece, part)
            order.append((piece, part))
            if len(order) - len(done) > 4:
                settle()

    def settle():
        piece, part = order[len(done)]
        done.append(piece)
        with scope(f"comb{part[0]}_{piece}"):
            for span in part:
                combine(piece, span)

    half_a, half_b = (0, 1), (2, 3)
    advance(half_a, 0, 2)
    with scope("y2"):
        take_stage(0, 0, 2)
        take_stage(0, 0, 3)
    if lines <= 4:
        between_hops(2, 4)
    advance(half_a, 2, 4)
    with scope("y3"):
        take_stage(0, 1, 2)
        take_stage(0, 1, 3)
    take_rest(2)
    take_rest(3)
    if lines <= 4:
        end_hops(4, 6)
        between_hops(4, 6)
    advance(half_b, 0, 4)
    if lines <= 4:
        between_hops(6, pieces)
        end_hops(6, pieces)
    states_sent()
    mixed_sent()
    advance(half_a, 4, 6)
    advance(half_b, 4, 6)
    lines_sent(1, lines)
    advance(half_a, 6, pieces)
    advance(half_b, 6, pieces)
    sides_sent()
    while len(order) - len(done) > 1:
        settle()
    with scope("combine_last"):
        settle()
        for span in range(spans):
            total_squares(span)
        for step in range(1, tp_size):
            square_copy(step).start()
    with scope("drain"):
        remote(
            partial_out, partial_in, partial_send.at[0], partial_recv.at[0, 0], {"lo": 1 - lo}
        ).wait_send()
    with scope("finish"):
        finish()
        for step in range(1, tp_size):
            square_copy(step).wait_send()


def layer(sizes, arrays):
    hi_size, inner_size, tp_size, per, tile, weight_tile = sizes
    rows, width = arrays[0].shape
    depth, columns = arrays[7].shape
    heads = width // HEAD_DIM
    groups = heads // per
    spans = rows // SPAN
    members = inner_size
    own_heads = heads // members
    kept = (groups + 1) // 2
    half_width = heads * tp_size // 2 * HEAD_DIM
    pieces = columns // weight_tile
    vmem = pl.BlockSpec(memory_space=pltpu.VMEM)
    anywhere = pl.BlockSpec(memory_space=pl.ANY)
    item = (HEAD_DIM + TAIL, HEAD_DIM)
    square = (HEAD_DIM, HEAD_DIM)
    bf16, f32 = jnp.bfloat16, jnp.float32
    dma = pltpu.SemaphoreType.DMA
    return pl.pallas_call(
        functools.partial(layer_kernel, sizes),
        in_specs=[anywhere] * 4 + [vmem] * 3 + [anywhere],
        out_specs=[vmem, vmem],
        out_shape=[
            pltpu.VMEM((rows, columns), bf16),
            pltpu.VMEM((spans, HEAD_DIM), f32),
        ],
        scratch_shapes=[
            pltpu.VMEM((hi_size * inner_size * depth, columns), bf16),
            pltpu.VMEM((hi_size * depth, columns), bf16),
            pltpu.VMEM((rows, width), bf16),
            pltpu.VMEM((rows, width), bf16),
            pltpu.VMEM((rows, width), bf16),
            pltpu.VMEM((rows, width), bf16),
            pltpu.VMEM((rows, width), f32),
            pltpu.VMEM((rows, width), f32),
            pltpu.VMEM((heads, max(8, spans), HEAD_DIM), f32),
            pltpu.VMEM((heads, max(1, spans - 1)) + square, bf16),
            pltpu.VMEM((heads,) + item, bf16),
            pltpu.VMEM((members, own_heads) + item, bf16),
            pltpu.VMEM((own_heads,) + square, bf16),
            pltpu.VMEM((own_heads,) + square, bf16),
            pltpu.VMEM((heads,) + square, bf16),
            pltpu.VMEM((heads,) + square, bf16),
            pltpu.VMEM((rows, width), f32),
            pltpu.VMEM((rows, width), bf16),
            pltpu.VMEM((rows, width), f32),
            pltpu.VMEM((rows, 2 * half_width + width), bf16),
            pltpu.VMEM((pieces, spans, SPAN, weight_tile), bf16),
            pltpu.VMEM((pieces, spans, SPAN, weight_tile), bf16),
            pltpu.VMEM((spans, SPAN, columns), f32),
            pltpu.VMEM((spans, SPAN, HEAD_DIM), f32),
            pltpu.VMEM((tp_size, max(8, spans), HEAD_DIM), f32),
            dma((5,)),
            dma((1,)),
            dma((members, own_heads)),
            dma((1,)),
            dma((own_heads,)),
            dma((1,)),
            dma((heads,)),
            dma((kept,)),
            dma((kept, spans)),
            dma((tp_size - 1, 2, kept)),
            dma((tp_size - 1, 2, kept, spans)),
            dma((2, 2 * hi_size - 1)),
            dma((2 * hi_size, pieces)),
            dma((inner_size - 1,)),
            dma((inner_size - 1, hi_size, pieces)),
            dma((1,)),
            dma((pieces, spans)),
            dma((tp_size - 1,)),
            dma((tp_size - 1,)),
        ],
        name="layer",
        compiler_params=pltpu.CompilerParams(
            collective_id=0, has_side_effects=True, vmem_limit_bytes=62800 * 1024
        ),
        cost_estimate=pl.CostEstimate(
            flops=rows * width * 10000, bytes_accessed=14 * rows * width, transcendentals=0
        ),
    )(*arrays)


def per_device(hi_size, inner_size, tp_size, *arrays):
    query, forget, value, gate, gap, surge, head_gain, matrix, branch_gain, residual = arrays
    per = inner_size * matrix.shape[0] // HEAD_DIM
    projected, scale = layer(
        (hi_size, inner_size, tp_size, per, 256, 128),
        (
            query,
            forget,
            value,
            gate,
            gap.reshape(-1, HEAD_DIM),
            surge,
            head_gain.reshape(1, HEAD_DIM),
            matrix,
        ),
    )
    columns = matrix.shape[1]
    gain_part = lax.dynamic_slice_in_dim(branch_gain, lax.axis_index("tp") * columns, columns)
    branch = projected.astype(jnp.float32) * scale.reshape(-1)[:, None] * gain_part
    return (residual.astype(jnp.float32) + branch).astype(jnp.bfloat16)


def solution(mesh):
    sp_size, tp_size = mesh.shape["sp"], mesh.shape["tp"]
    sp = ("hi", "lo", "inner")
    placed = (
        P(sp, "tp"),
        P(sp, "tp"),
        P(sp, "tp"),
        P(sp, "tp"),
        P(),
        P("tp", sp),
        P(),
        P(sp, "tp"),
        P(),
        P(sp, "tp"),
    )

    def whole(*arrays):
        inner = max(2, HEAD_DIM * sp_size // arrays[7].shape[0])
        hi = sp_size // (2 * inner)
        devices = mesh.devices.reshape(hi, 2, inner, tp_size)
        paired = Mesh(devices, ("hi", "lo", "inner", "tp"))
        return jax.shard_map(
            functools.partial(per_device, hi, inner, tp_size),
            mesh=paired,
            in_specs=placed,
            out_specs=P(sp, "tp"),
            check_vma=False,
        )(*arrays)

    return whole
```

```python
import functools

import jax
import jax.numpy as jnp
from jax import lax
from jax.experimental import pallas as pl
from jax.experimental.pallas import tpu as pltpu
from jax.sharding import Mesh
from jax.sharding import PartitionSpec as P

HEAD_DIM = 128
SPAN = 128
TAIL = 16
EPSILON = 1e-06
NT = (((1,), (1,)), ((), ()))
TN = (((0,), (0,)), ((), ()))
NN = (((1,), (0,)), ((), ()))
MESH_ID = pl.DeviceIdType.MESH


def dot(a, b, dims=NN):
    return lax.dot_general(a, b, dims, preferred_element_type=jnp.float32)


def lower_triangle():
    rows = lax.broadcasted_iota(jnp.int32, (SPAN, SPAN), 0)
    columns = lax.broadcasted_iota(jnp.int32, (SPAN, SPAN), 1)
    return rows >= columns


def diagonal():
    rows = lax.broadcasted_iota(jnp.int32, (SPAN, SPAN), 0)
    columns = lax.broadcasted_iota(jnp.int32, (SPAN, SPAN), 1)
    return rows == columns


def silu(logits):
    return logits / (1.0 + jnp.exp(-logits))


def decays(logits, gap, surge, causal):
    keys = gap / (1.0 + jnp.exp(logits.astype(jnp.float32)))
    series = keys * (1.0 / 7.0) + (1.0 / 6.0)
    for order in (5, 4, 3, 2):
        series = series * keys + (1.0 / order)
    logs = -(series * keys + 1.0) * keys
    high = logs.astype(jnp.bfloat16)
    low = (logs - high.astype(jnp.float32)).astype(jnp.bfloat16)
    ones = causal.astype(jnp.bfloat16)
    surged = jnp.sum(jnp.where(causal, surge, 0.0), axis=1, keepdims=True)
    return keys, dot(ones, high) + dot(ones, low) + surged


def layer_kernel(
    sizes,
    query_in,
    forget_in,
    value_in,
    gate_in,
    gap_ref,
    surge_ref,
    gain_ref,
    weight_in,
    projected_ref,
    scale_ref,
    whole_weight,
    relay,
    query_ref,
    forget_ref,
    value_ref,
    gate_ref,
    running_ref,
    keys_ref,
    base_ref,
    starts_ref,
    state_out,
    gathered,
    chain_in,
    chain_out,
    deliver_out,
    carried,
    local_ref,
    reach_ref,
    gated_ref,
    mixed_ref,
    partial_out,
    partial_in,
    total_ref,
    sums_ref,
    squares_ref,
    load_sems,
    gather_send,
    gather_recv,
    chain_send,
    chain_recv,
    deliver_send,
    deliver_recv,
    swap_send,
    swap_recv,
    tp_send,
    tp_recv,
    line_send,
    line_recv,
    side_send,
    side_recv,
    partial_send,
    partial_recv,
    square_send,
    square_recv,
):
    hi_size, inner_size, tp_size, per, tile, weight_tile = sizes
    rows, width = query_in.shape
    depth, columns = weight_in.shape
    heads = width // HEAD_DIM
    spans = rows // SPAN
    groups = heads // per
    half_width = heads * tp_size // 2 * HEAD_DIM
    members = inner_size
    lines = 2 * hi_size
    own_heads = heads // members
    tiles = columns // tile
    pieces = columns // weight_tile
    hi, lo, inner, tp = (lax.axis_index(a) for a in ("hi", "lo", "inner", "tp"))
    member = inner
    line = hi * 2 + lo
    strides = []
    by = tp_size // 2
    while by >= 1:
        strides.append(by)
        by //= 2

    def member_at(index):
        return {"inner": index}

    def on_line(index):
        return {"hi": index // 2, "lo": index % 2}

    def flipped(index, by):
        return index + by - 2 * by * ((index // by) % 2)

    def remote(source, target, send, recv, device):
        return pltpu.make_async_remote_copy(
            src_ref=source,
            dst_ref=target,
            send_sem=send,
            recv_sem=recv,
            device_id=device,
            device_id_type=MESH_ID,
        )

    def span_rows(span):
        return pl.ds(span * SPAN, SPAN)

    def lanes_of(head):
        return pl.ds(pl.multiple_of(head * HEAD_DIM, HEAD_DIM), HEAD_DIM)

    def slot_rows(block_hi, block_inner):
        return pl.ds(pl.multiple_of((block_hi * inner_size + block_inner) * depth, depth), depth)

    loads = [
        pltpu.make_async_copy(source, target, load_sems.at[number])
        for number, (source, target) in enumerate(
            (
                (weight_in, whole_weight.at[slot_rows(hi, inner)]),
                (forget_in, forget_ref),
                (value_in, value_ref),
                (query_in, query_ref),
                (gate_in, gate_ref),
            )
        )
    ]
    for load in loads:
        load.start()

    barrier = pltpu.get_barrier_semaphore()

    peers = members - 1 + tp_size - 1
    for step in range(1, members):
        pl.semaphore_signal(
            barrier,
            inc=1,
            device_id=member_at((member + step) % members),
            device_id_type=MESH_ID,
        )
    for step in range(1, tp_size):
        pl.semaphore_signal(
            barrier, inc=1, device_id={"tp": (tp + step) % tp_size}, device_id_type=MESH_ID
        )
    for step in (1, -1):
        there = line + step
        inside = (there >= 0) & (there < lines)

        @pl.when(inside)
        def _():
            pl.semaphore_signal(barrier, inc=1, device_id=on_line(there), device_id_type=MESH_ID)

        peers = peers + jnp.where(inside, 1, 0)
    pl.semaphore_wait(barrier, peers)

    def piece_lanes(piece):
        return pl.ds(piece * weight_tile, weight_tile)

    def weight_block(block_hi, block_inner, piece):
        return whole_weight.at[slot_rows(block_hi, block_inner), piece_lanes(piece)]

    def step_of(way):
        return 1 if way == 0 else -1

    def line_block(origin, distance, piece):
        block_hi = origin // 2
        if distance % 2 == 0:
            return weight_block(block_hi, inner, piece)
        return relay.at[
            pl.ds(pl.multiple_of(block_hi * depth, depth), depth), piece_lanes(piece)
        ]

    def line_copy(way, hop, piece):
        origin = line - step_of(way) * (hop - 1)
        return remote(
            line_block(origin, hop - 1, piece),
            line_block(origin, hop, piece),
            line_send.at[way, hop - 1],
            line_recv.at[origin, piece],
            on_line(line + step_of(way)),
        )

    def line_arrival(origin, piece):
        block = weight_block(hi, inner, piece)
        return remote(
            block, block, line_send.at[0, 0], line_recv.at[origin, piece], on_line(origin)
        )

    def line_sent(way, hop):
        block = whole_weight.at[slot_rows(hi, inner)]
        return remote(
            block,
            block,
            line_send.at[way, hop - 1],
            line_recv.at[0, 0],
            on_line(line + step_of(way)),
        )

    def inside(index):
        return (index >= 0) & (index < lines)

    def sends(way, hop):
        step = step_of(way)
        last = line + step * (1 + hop % 2)
        return inside(line - step * (hop - 1)) & inside(last)

    def receives(way, hop):
        step = step_of(way)
        return inside(line - step * hop) & inside(line + step * (hop % 2))

    def side_copy(reach, block_hi, piece):
        block = weight_block(block_hi, inner, piece)
        return remote(
            block,
            block,
            side_send.at[reach - 1],
            side_recv.at[reach - 1, block_hi, piece],
            {"inner": (inner + reach) % inner_size},
        )

    def start_line(way, piece):
        @pl.when(sends(way, 1))
        def _():
            line_copy(way, 1, piece).start()

    def start_side(piece):
        for reach in range(1, inner_size):
            side_copy(reach, hi, piece).start()

    def take_hop(hop, way, piece):
        if hop >= lines:
            return
        origin = line - step_of(way) * hop

        @pl.when(receives(way, hop))
        def _():
            line_arrival(origin, piece).wait_recv()
            if hop % 2 == 0:
                for reach in range(1, inner_size):
                    side_copy(reach, origin // 2, piece).start()

        if hop + 1 < lines:

            @pl.when(sends(way, hop + 1))
            def _():
                line_copy(way, hop + 1, piece).start()

    def take_sides(piece):
        for reach in range(1, inner_size):
            for block_hi in range(hi_size):
                side_copy(reach, block_hi, piece).wait_recv()

    def sides_sent():
        for reach in range(1, inner_size):
            remote(
                whole_weight.at[pl.ds(0, hi_size * depth)],
                whole_weight.at[pl.ds(0, hi_size * depth)],
                side_send.at[reach - 1],
                side_recv.at[0, 0, 0],
                {"inner": (inner + reach) % inner_size},
            ).wait_send()

    def state_copy(head):
        return remote(
            state_out.at[head],
            gathered.at[member, head % own_heads],
            gather_send.at[0],
            gather_recv.at[member, head % own_heads],
            member_at(head // own_heads),
        )

    def state_arrival(index, number):
        return remote(
            state_out.at[0],
            gathered.at[index, number],
            gather_send.at[0],
            gather_recv.at[index, number],
            member_at(index),
        )

    def chain_copy(number):
        return remote(
            chain_out.at[number],
            chain_in.at[number],
            chain_send.at[0],
            chain_recv.at[number],
            on_line(line + 1),
        )

    def deliver_copy(index, number):
        head = member * own_heads + number
        return remote(
            deliver_out.at[index * own_heads + number],
            carried.at[head],
            deliver_send.at[0],
            deliver_recv.at[head],
            member_at(index),
        )

    def deliver_arrival(head):
        return remote(
            deliver_out.at[0],
            carried.at[head],
            deliver_send.at[0],
            deliver_recv.at[head],
            member_at(head // own_heads),
        )

    def head_state(head):
        causal = lower_triangle()
        gap = gap_ref[pl.ds(tp * heads + head, 1), :]
        lanes = lanes_of(head)
        this_head = lax.broadcasted_iota(jnp.int32, (heads, SPAN), 0) == head
        state = jnp.zeros((HEAD_DIM, HEAD_DIM), jnp.float32)
        base = jnp.zeros((1, HEAD_DIM), jnp.float32)
        for span in range(spans):
            part = span_rows(span)
            surge = jnp.sum(jnp.where(this_head, surge_ref[:, part], 0.0), axis=0, keepdims=True)
            keys, running = decays(forget_ref[part, lanes], gap, surge, causal)
            keys_ref[part, lanes] = keys
            running_ref[part, lanes] = running
            base_ref[head, span : span + 1, :] = base
            if span > 0:
                starts_ref[head, span - 1] = state.astype(jnp.bfloat16)
            ending = running[SPAN - 1 : SPAN, :]
            kept = (keys * jnp.exp(ending - running)).astype(jnp.bfloat16)
            state = state * jnp.exp(ending) + dot(value_ref[part, lanes], kept, TN)
            base = base + ending
        decay = jnp.exp(base)
        high = decay.astype(jnp.bfloat16).astype(jnp.float32)
        first = lax.broadcasted_iota(jnp.int32, (TAIL, HEAD_DIM), 0) == 0
        item = state.astype(jnp.bfloat16)
        tail = jnp.where(first, high, decay - high).astype(jnp.bfloat16)
        state_out[head, 0:HEAD_DIM, :] = item
        state_out[head, HEAD_DIM:, :] = tail

    def state_body(turn, carry):
        pair = [(turn * 2 + number + (member + 1) * own_heads) % heads for number in range(2)]
        for head in pair:
            head_state(head)
        for head in pair:
            owner = head // own_heads

            @pl.when(owner == member)
            def _():
                gathered[member, head % own_heads] = state_out[head]

            @pl.when(owner != member)
            def _():
                state_copy(head).start()

        return carry

    def chain_states():
        @pl.when(line == 0)
        def _():
            chain_in[...] = jnp.zeros_like(chain_in)

        def body(number, carry):
            for index in range(members):

                @pl.when(member != index)
                def _():
                    state_arrival(index, number).wait_recv()

            @pl.when(line > 0)
            def _():
                chain_copy(number).wait_recv()

            state = chain_in[number].astype(jnp.float32)
            for index in range(members):
                deliver_out[index * own_heads + number] = state.astype(jnp.bfloat16)
                tail = gathered[index, number, HEAD_DIM:, :].astype(jnp.float32)
                item = gathered[index, number, 0:HEAD_DIM, :].astype(jnp.float32)
                state = state * (tail[0:1, :] + tail[1:2, :]) + item
            chain_out[number] = state.astype(jnp.bfloat16)

            @pl.when(line + 1 < lines)
            def _():
                chain_copy(number).start()

            for index in range(members):

                @pl.when(member != index)
                def _():
                    deliver_copy(index, number).start()

            carried[member * own_heads + number] = deliver_out[member * own_heads + number]
            return carry

        lax.fori_loop(0, own_heads, body, 0)

    def take_states():
        def body(head, carry):
            @pl.when(head // own_heads != member)
            def _():
                deliver_arrival(head).wait_recv()

            return carry

        lax.fori_loop(0, heads, body, 0)

    gain = gain_ref[...]

    def local_body(head, carry):
        causal = lower_triangle()
        lanes = lanes_of(head)
        middle = SPAN // 2
        for span in range(spans):
            part = span_rows(span)
            running = running_ref[part, lanes]
            anchor = running[middle - 1 : middle, :]
            queries = silu(query_ref[part, lanes].astype(jnp.float32)) * (HEAD_DIM**-0.5)
            reach = queries * jnp.exp(running - anchor)
            back = keys_ref[part, lanes] * jnp.exp(anchor - running)
            scores = dot(reach.astype(jnp.bfloat16), back.astype(jnp.bfloat16), NT)
            scores = jnp.where(causal, scores, 0.0).astype(jnp.bfloat16)
            out = dot(scores, value_ref[part, lanes])
            if span > 0:
                out = out + dot(
                    (reach * jnp.exp(anchor)).astype(jnp.bfloat16), starts_ref[head, span - 1], NT
                )
            local_ref[part, lanes] = out
            base = base_ref[head, span : span + 1, :]
            reach_ref[part, lanes] = (reach * jnp.exp(anchor + base)).astype(jnp.bfloat16)
            gated_ref[part, lanes] = gain * silu(gate_ref[part, lanes].astype(jnp.float32))
        return carry

    def keeps(index, group):
        return (index * groups + group) % 2 == lo

    def group_lanes(index, group, which):
        start = which * half_width + (index * groups + group) // 2 * per * HEAD_DIM
        return pl.ds(pl.multiple_of(start, HEAD_DIM), per * HEAD_DIM)

    def swap_copy(group, span):
        start = 2 * half_width + group * per * HEAD_DIM
        return remote(
            mixed_ref.at[span_rows(span), pl.ds(start, per * HEAD_DIM)],
            mixed_ref.at[span_rows(span), group_lanes(tp, group, 1)],
            swap_send.at[group // 2],
            swap_recv.at[group // 2, span],
            {"lo": 1 - lo},
        )

    def origin_of(index, mask):
        for bit, by in enumerate(strides):
            if (mask >> bit) & 1:
                index = flipped(index, by)
        return index

    def tp_copy(stage, which, mask, group, span):
        block = mixed_ref.at[span_rows(span), group_lanes(origin_of(tp, mask), group, which)]
        return remote(
            block,
            block,
            tp_send.at[(1 << stage) - 1 + mask, which, group // 2],
            tp_recv.at[(1 << stage) - 1 + mask, which, group // 2, span],
            {"tp": flipped(tp, strides[stage])},
        )

    def mix(span):
        part = span_rows(span)
        for head in range(heads):
            lanes = lanes_of(head)
            out = local_ref[part, lanes] + dot(reach_ref[part, lanes], carried[head], NT)
            mean_sq = jnp.mean(out * out, axis=1, keepdims=True)
            mixed = out * lax.rsqrt(mean_sq + EPSILON) * gated_ref[part, lanes]
            group = head // per
            kept_start = (tp * groups + group) // 2 * per * HEAD_DIM + head % per * HEAD_DIM
            away_start = 2 * half_width + head * HEAD_DIM
            start = jnp.where(keeps(tp, group), kept_start, away_start)
            mixed_ref[part, pl.ds(pl.multiple_of(start, HEAD_DIM), HEAD_DIM)] = mixed.astype(
                jnp.bfloat16
            )

    def send_away(span):
        for group in range(groups):

            @pl.when(jnp.logical_not(keeps(tp, group)))
            def _():
                swap_copy(group, span).start()

    def send_kept(span):
        for group in range(groups):

            @pl.when(keeps(tp, group))
            def _():
                for stage in range(len(strides)):
                    tp_copy(stage, 0, 0, group, span).start()

    def take_swap(span):
        for group in range(groups):

            @pl.when(keeps(tp, group))
            def _():
                swap_copy(group, span).wait_recv()
                for stage in range(len(strides)):
                    tp_copy(stage, 1, 0, group, span).start()

    def take_stage(stage, which, span):
        peer = flipped(tp, strides[stage])
        for mask in range(1 << stage):
            for group in range(groups):

                @pl.when(keeps(origin_of(peer, mask), group))
                def _():
                    tp_copy(stage, which, mask, group, span).wait_recv()
                    for later in range(stage + 1, len(strides)):
                        tp_copy(later, which, mask | (1 << stage), group, span).start()

    def partial_copy(piece, span):
        return remote(
            partial_out.at[piece, span],
            partial_in.at[piece, span],
            partial_send.at[0],
            partial_recv.at[piece, span],
            {"lo": 1 - lo},
        )

    def both(span, start, depth):
        part = span_rows(span)
        return jnp.concatenate(
            [mixed_ref[part, half_width : 2 * half_width], mixed_ref[part, 0:half_width]], axis=0
        )

    def multiply(piece, part):
        lanes = piece_lanes(piece)
        right = whole_weight[:, lanes]
        for span in part:
            total = dot(both(span, 0, half_width), right)
            partial_out[piece, span] = total[0:SPAN].astype(jnp.bfloat16)
            partial_copy(piece, span).start()
            total_ref[span, :, lanes] = total[SPAN:]

    def square_copy(step):
        return remote(
            squares_ref.at[tp],
            squares_ref.at[tp],
            square_send.at[step - 1],
            square_recv.at[step - 1],
            {"tp": (tp + step) % tp_size},
        )

    def combine(piece, span):
        lanes = pl.ds(piece * weight_tile, weight_tile)
        partial_copy(piece, span).wait_recv()
        total = total_ref[span, :, lanes] + partial_in[piece, span].astype(jnp.float32)
        rounded = total.astype(jnp.bfloat16)
        projected_ref[span_rows(span), lanes] = rounded
        branch = rounded.astype(jnp.float32)
        branch = branch * branch
        squares = branch[:, 0:HEAD_DIM]
        for start in range(HEAD_DIM, weight_tile, HEAD_DIM):
            squares = squares + branch[:, start : start + HEAD_DIM]
        if piece > 0:
            squares = squares + sums_ref[span]
        sums_ref[span] = squares

    def total_squares(span):
        column = jnp.sum(sums_ref[span], axis=1, keepdims=True)
        row = jnp.sum(jnp.where(diagonal(), column, 0.0), axis=0, keepdims=True)
        squares_ref[tp, span : span + 1, :] = row

    def finish():
        for step in range(1, tp_size):
            square_copy(step).wait_recv()
        total = squares_ref[0, 0:spans, :]
        for index in range(1, tp_size):
            total = total + squares_ref[index, 0:spans, :]
        scale_ref[...] = lax.rsqrt(total * (1.0 / (columns * tp_size)) + EPSILON)

    def lines_sent(first, last):
        for hop in range(first, last):
            for way in (0, 1):

                @pl.when(sends(way, hop))
                def _():
                    line_sent(way, hop).wait_send()

    def states_sent():
        others = (members - 1) * own_heads
        next_member = member_at((member + 1) % members)
        pltpu.make_async_remote_copy(
            src_ref=state_out.at[pl.ds(0, others)],
            dst_ref=state_out.at[pl.ds(0, others)],
            send_sem=gather_send.at[0],
            recv_sem=gather_recv.at[0, 0],
            device_id=next_member,
            device_id_type=MESH_ID,
        ).wait_send()
        pltpu.make_async_remote_copy(
            src_ref=deliver_out.at[pl.ds(0, others)],
            dst_ref=deliver_out.at[pl.ds(0, others)],
            send_sem=deliver_send.at[0],
            recv_sem=deliver_recv.at[0],
            device_id=next_member,
            device_id_type=MESH_ID,
        ).wait_send()

        @pl.when(line + 1 < lines)
        def _():
            remote(
                chain_out, chain_in, chain_send.at[0], chain_recv.at[0], on_line(line + 1)
            ).wait_send()

    def swaps_sent():
        for group in range(groups):
            block = mixed_ref.at[:, group_lanes(tp, group, 0)]

            @pl.when(jnp.logical_not(keeps(tp, group)))
            def _():
                remote(
                    block, block, swap_send.at[group // 2], swap_recv.at[0, 0], {"lo": 1 - lo}
                ).wait_send()

    def mixed_sent():
        for group in range(groups):
            block = mixed_ref.at[:, group_lanes(tp, group, 0)]

            for stage in range(len(strides)):
                for which in (0, 1):
                    for mask in range(1 << stage):

                        @pl.when(keeps(origin_of(tp, mask), group))
                        def _():
                            remote(
                                block,
                                block,
                                tp_send.at[(1 << stage) - 1 + mask, which, group // 2],
                                tp_recv.at[0, 0, 0, 0],
                                {"tp": flipped(tp, strides[stage])},
                            ).wait_send()

    early = line < 2
    ends = (line == 0) | (line == lines - 1)
    between = jnp.logical_not(ends)
    scope = jax.named_scope

    def local():
        with scope("local"):
            lax.fori_loop(0, heads, local_body, 0)

    def hop_pieces(hop, way, first, last):
        with scope(f"hop{hop}_{way}_{first}"):
            for piece in range(first, last):
                take_hop(hop, way, piece)

    low = line < lines // 2

    def outward(first, last):
        @pl.when(low)
        def _():
            hop_pieces(1, 1, first, last)

        @pl.when(jnp.logical_not(low))
        def _():
            hop_pieces(1, 0, first, last)

    def inward(first, last):
        @pl.when(low)
        def _():
            hop_pieces(1, 0, first, last)

        @pl.when(jnp.logical_not(low))
        def _():
            hop_pieces(1, 1, first, last)

    def own_sides(first, last):
        for piece in range(first, last):
            start_side(piece)

    loads[0].wait()
    for piece in range(pieces):
        if piece < 3:
            start_line(0, piece)
        elif piece == 3:

            @pl.when(line > 0)
            def _():
                start_line(0, piece)

        start_line(1, piece)
    own_sides(0, 1)
    loads[1].wait()
    loads[2].wait()
    with scope("state"):
        lax.fori_loop(0, heads // 2, state_body, 0)
    own_sides(1, 3)
    outward(0, 2)

    @pl.when(jnp.logical_not(low))
    def _():
        hop_pieces(1, 1, 0, 2)

    loads[3].wait()
    loads[4].wait()

    @pl.when(jnp.logical_not(early))
    def _():
        local()

    with scope("chain"):
        chain_states()

    @pl.when(line == 0)
    def _():
        for piece in range(3, 6):
            start_line(0, piece)

    @pl.when(line > 0)
    def _():
        for piece in range(4, pieces):
            start_line(0, piece)

    @pl.when(ends)
    def _():
        own_sides(3, 6)

    @pl.when(between)
    def _():
        own_sides(3, pieces)

    outward(2, 4)

    @pl.when(early)
    def _():
        local()

    def end_hops(first, last):
        @pl.when(ends)
        def _():
            hop_pieces(2, 1, first, last)
            hop_pieces(2, 0, first, last)

    def between_hops(first, last):
        @pl.when(between)
        def _():
            hop_pieces(2, 1, first, last)
            hop_pieces(2, 0, first, last)


    @pl.when(low)
    def _():
        hop_pieces(1, 0, 0, 2)

    inward(2, 4)
    with scope("take_states"):
        take_states()
    with scope("mix"):
        for span in range(spans):
            mix(span)
            send_away(span)
            if span < 2:
                send_kept(span)


    end_hops(0, 4)
    keeper = keeps(tp, 0)

    @pl.when(jnp.logical_not(keeper))
    def _():
        between_hops(0, 2)

    with scope("swap01"):
        for span in range(2):
            take_swap(span)
            send_kept(span + 2)

    with scope("swapsent"):
        swaps_sent()

    @pl.when(line == 0)
    def _():
        for piece in range(6, pieces):
            start_line(0, piece)

    outward(4, 6)

    @pl.when(jnp.logical_not(low))
    def _():
        hop_pieces(1, 1, 4, pieces)


    @pl.when(keeper)
    def _():
        between_hops(0, 2)


    @pl.when(low)
    def _():
        hop_pieces(1, 0, 4, 6)

    def take_rest(span):
        with scope(f"take{span}"):
            for stage in range(1, len(strides)):
                for which in (0, 1):
                    take_stage(stage, which, span)

    with scope("y0"):
        take_stage(0, 0, 0)
        take_stage(0, 0, 1)
        take_swap(2)
        take_swap(3)
    outward(6, pieces)

    @pl.when(ends)
    def _():
        own_sides(6, pieces)

    if lines <= 4:
        between_hops(2, 4)
    with scope("y1"):
        take_stage(0, 1, 0)
        take_stage(0, 1, 1)
    take_rest(0)
    take_rest(1)
    @pl.when(low)
    def _():
        hop_pieces(1, 0, 6, pieces)

    if lines > 4:
        between_hops(2, pieces)
        end_hops(4, pieces)
    for hop in range(3, lines):
        for way in (0, 1):
            hop_pieces(hop, way, 0, pieces)
    done = []
    order = []

    def advance(part, first, last):
        for piece in range(first, last):
            if not any(piece == other for other, _ in order):
                with scope(f"sides{piece}"):
                    take_sides(piece)
            with scope(f"mult{part[0]}_{piece}"):
                multiply(piece, part)
            order.append((piece, part))
            if len(order) - len(done) > 4:
                settle()

    def settle():
        piece, part = order[len(done)]
        done.append(piece)
        with scope(f"comb{part[0]}_{piece}"):
            for span in part:
                combine(piece, span)

    half_a, half_b = (0, 1), (2, 3)
    advance(half_a, 0, 2)
    with scope("y2"):
        take_stage(0, 0, 2)
        take_stage(0, 0, 3)
    if lines <= 4:
        end_hops(4, 6)
        between_hops(4, 6)
    advance(half_a, 2, 4)
    with scope("y3"):
        take_stage(0, 1, 2)
        take_stage(0, 1, 3)
    take_rest(2)
    take_rest(3)
    if lines <= 4:
        between_hops(6, pieces)
        end_hops(6, pieces)
    advance(half_b, 0, 4)
    states_sent()
    mixed_sent()
    advance(half_a, 4, 6)
    advance(half_b, 4, 6)
    lines_sent(1, lines)
    advance(half_a, 6, pieces)
    advance(half_b, 6, pieces)
    sides_sent()
    while len(order) - len(done) > 1:
        settle()
    with scope("combine_last"):
        settle()
        for span in range(spans):
            total_squares(span)
        for step in range(1, tp_size):
            square_copy(step).start()
    with scope("drain"):
        remote(
            partial_out, partial_in, partial_send.at[0], partial_recv.at[0, 0], {"lo": 1 - lo}
        ).wait_send()
    with scope("finish"):
        finish()
        for step in range(1, tp_size):
            square_copy(step).wait_send()


def layer(sizes, arrays):
    hi_size, inner_size, tp_size, per, tile, weight_tile = sizes
    rows, width = arrays[0].shape
    depth, columns = arrays[7].shape
    heads = width // HEAD_DIM
    groups = heads // per
    spans = rows // SPAN
    members = inner_size
    own_heads = heads // members
    kept = (groups + 1) // 2
    half_width = heads * tp_size // 2 * HEAD_DIM
    pieces = columns // weight_tile
    vmem = pl.BlockSpec(memory_space=pltpu.VMEM)
    anywhere = pl.BlockSpec(memory_space=pl.ANY)
    item = (HEAD_DIM + TAIL, HEAD_DIM)
    square = (HEAD_DIM, HEAD_DIM)
    bf16, f32 = jnp.bfloat16, jnp.float32
    dma = pltpu.SemaphoreType.DMA
    return pl.pallas_call(
        functools.partial(layer_kernel, sizes),
        in_specs=[anywhere] * 4 + [vmem] * 3 + [anywhere],
        out_specs=[vmem, vmem],
        out_shape=[
            pltpu.VMEM((rows, columns), bf16),
            pltpu.VMEM((spans, HEAD_DIM), f32),
        ],
        scratch_shapes=[
            pltpu.VMEM((hi_size * inner_size * depth, columns), bf16),
            pltpu.VMEM((hi_size * depth, columns), bf16),
            pltpu.VMEM((rows, width), bf16),
            pltpu.VMEM((rows, width), bf16),
            pltpu.VMEM((rows, width), bf16),
            pltpu.VMEM((rows, width), bf16),
            pltpu.VMEM((rows, width), f32),
            pltpu.VMEM((rows, width), f32),
            pltpu.VMEM((heads, max(8, spans), HEAD_DIM), f32),
            pltpu.VMEM((heads, max(1, spans - 1)) + square, bf16),
            pltpu.VMEM((heads,) + item, bf16),
            pltpu.VMEM((members, own_heads) + item, bf16),
            pltpu.VMEM((own_heads,) + square, bf16),
            pltpu.VMEM((own_heads,) + square, bf16),
            pltpu.VMEM((heads,) + square, bf16),
            pltpu.VMEM((heads,) + square, bf16),
            pltpu.VMEM((rows, width), f32),
            pltpu.VMEM((rows, width), bf16),
            pltpu.VMEM((rows, width), f32),
            pltpu.VMEM((rows, 2 * half_width + width), bf16),
            pltpu.VMEM((pieces, spans, SPAN, weight_tile), bf16),
            pltpu.VMEM((pieces, spans, SPAN, weight_tile), bf16),
            pltpu.VMEM((spans, SPAN, columns), f32),
            pltpu.VMEM((spans, SPAN, HEAD_DIM), f32),
            pltpu.VMEM((tp_size, max(8, spans), HEAD_DIM), f32),
            dma((5,)),
            dma((1,)),
            dma((members, own_heads)),
            dma((1,)),
            dma((own_heads,)),
            dma((1,)),
            dma((heads,)),
            dma((kept,)),
            dma((kept, spans)),
            dma((tp_size - 1, 2, kept)),
            dma((tp_size - 1, 2, kept, spans)),
            dma((2, 2 * hi_size - 1)),
            dma((2 * hi_size, pieces)),
            dma((inner_size - 1,)),
            dma((inner_size - 1, hi_size, pieces)),
            dma((1,)),
            dma((pieces, spans)),
            dma((tp_size - 1,)),
            dma((tp_size - 1,)),
        ],
        name="layer",
        compiler_params=pltpu.CompilerParams(
            collective_id=0, has_side_effects=True, vmem_limit_bytes=62800 * 1024
        ),
        cost_estimate=pl.CostEstimate(
            flops=rows * width * 10000, bytes_accessed=14 * rows * width, transcendentals=0
        ),
    )(*arrays)


def per_device(hi_size, inner_size, tp_size, *arrays):
    query, forget, value, gate, gap, surge, head_gain, matrix, branch_gain, residual = arrays
    per = inner_size * matrix.shape[0] // HEAD_DIM
    projected, scale = layer(
        (hi_size, inner_size, tp_size, per, 256, 128),
        (
            query,
            forget,
            value,
            gate,
            gap.reshape(-1, HEAD_DIM),
            surge,
            head_gain.reshape(1, HEAD_DIM),
            matrix,
        ),
    )
    columns = matrix.shape[1]
    gain_part = lax.dynamic_slice_in_dim(branch_gain, lax.axis_index("tp") * columns, columns)
    branch = projected.astype(jnp.float32) * scale.reshape(-1)[:, None] * gain_part
    return (residual.astype(jnp.float32) + branch).astype(jnp.bfloat16)


def solution(mesh):
    sp_size, tp_size = mesh.shape["sp"], mesh.shape["tp"]
    sp = ("hi", "lo", "inner")
    placed = (
        P(sp, "tp"),
        P(sp, "tp"),
        P(sp, "tp"),
        P(sp, "tp"),
        P(),
        P("tp", sp),
        P(),
        P(sp, "tp"),
        P(),
        P(sp, "tp"),
    )

    def whole(*arrays):
        inner = max(2, HEAD_DIM * sp_size // arrays[7].shape[0])
        hi = sp_size // (2 * inner)
        devices = mesh.devices.reshape(hi, 2, inner, tp_size)
        paired = Mesh(devices, ("hi", "lo", "inner", "tp"))
        return jax.shard_map(
            functools.partial(per_device, hi, inner, tp_size),
            mesh=paired,
            in_specs=placed,
            out_specs=P(sp, "tp"),
            check_vma=False,
        )(*arrays)

    return whole
```

```python
import functools

import jax
import jax.numpy as jnp
from jax import lax
from jax.experimental import pallas as pl
from jax.experimental.pallas import tpu as pltpu
from jax.sharding import Mesh
from jax.sharding import PartitionSpec as P

HEAD_DIM = 128
SPAN = 128
TAIL = 16
EPSILON = 1e-06
NT = (((1,), (1,)), ((), ()))
TN = (((0,), (0,)), ((), ()))
NN = (((1,), (0,)), ((), ()))
MESH_ID = pl.DeviceIdType.MESH


def dot(a, b, dims=NN):
    return lax.dot_general(a, b, dims, preferred_element_type=jnp.float32)


def lower_triangle():
    rows = lax.broadcasted_iota(jnp.int32, (SPAN, SPAN), 0)
    columns = lax.broadcasted_iota(jnp.int32, (SPAN, SPAN), 1)
    return rows >= columns


def diagonal():
    rows = lax.broadcasted_iota(jnp.int32, (SPAN, SPAN), 0)
    columns = lax.broadcasted_iota(jnp.int32, (SPAN, SPAN), 1)
    return rows == columns


def silu(logits):
    return logits / (1.0 + jnp.exp(-logits))


def decays(logits, gap, surge, causal):
    keys = gap / (1.0 + jnp.exp(logits.astype(jnp.float32)))
    series = keys * (1.0 / 7.0) + (1.0 / 6.0)
    for order in (5, 4, 3, 2):
        series = series * keys + (1.0 / order)
    logs = -(series * keys + 1.0) * keys
    high = logs.astype(jnp.bfloat16)
    low = (logs - high.astype(jnp.float32)).astype(jnp.bfloat16)
    ones = causal.astype(jnp.bfloat16)
    surged = jnp.sum(jnp.where(causal, surge, 0.0), axis=1, keepdims=True)
    return keys, dot(ones, high) + dot(ones, low) + surged


def layer_kernel(
    sizes,
    query_in,
    forget_in,
    value_in,
    gate_in,
    gap_ref,
    surge_ref,
    gain_ref,
    weight_in,
    projected_ref,
    scale_ref,
    whole_weight,
    relay,
    query_ref,
    forget_ref,
    value_ref,
    gate_ref,
    running_ref,
    keys_ref,
    base_ref,
    starts_ref,
    state_out,
    gathered,
    chain_in,
    chain_out,
    deliver_out,
    carried,
    local_ref,
    reach_ref,
    gated_ref,
    mixed_ref,
    partial_out,
    partial_in,
    total_ref,
    sums_ref,
    squares_ref,
    load_sems,
    gather_send,
    gather_recv,
    chain_send,
    chain_recv,
    deliver_send,
    deliver_recv,
    swap_send,
    swap_recv,
    tp_send,
    tp_recv,
    line_send,
    line_recv,
    side_send,
    side_recv,
    partial_send,
    partial_recv,
    square_send,
    square_recv,
):
    hi_size, inner_size, tp_size, per, tile, weight_tile = sizes
    rows, width = query_in.shape
    depth, columns = weight_in.shape
    heads = width // HEAD_DIM
    spans = rows // SPAN
    groups = heads // per
    half_width = heads * tp_size // 2 * HEAD_DIM
    members = inner_size
    lines = 2 * hi_size
    own_heads = heads // members
    tiles = columns // tile
    pieces = columns // weight_tile
    hi, lo, inner, tp = (lax.axis_index(a) for a in ("hi", "lo", "inner", "tp"))
    member = inner
    line = hi * 2 + lo
    strides = []
    by = tp_size // 2
    while by >= 1:
        strides.append(by)
        by //= 2

    def member_at(index):
        return {"inner": index}

    def on_line(index):
        return {"hi": index // 2, "lo": index % 2}

    def flipped(index, by):
        return index + by - 2 * by * ((index // by) % 2)

    def remote(source, target, send, recv, device):
        return pltpu.make_async_remote_copy(
            src_ref=source,
            dst_ref=target,
            send_sem=send,
            recv_sem=recv,
            device_id=device,
            device_id_type=MESH_ID,
        )

    def span_rows(span):
        return pl.ds(span * SPAN, SPAN)

    def lanes_of(head):
        return pl.ds(pl.multiple_of(head * HEAD_DIM, HEAD_DIM), HEAD_DIM)

    def slot_rows(block_hi, block_inner):
        return pl.ds(pl.multiple_of((block_hi * inner_size + block_inner) * depth, depth), depth)

    loads = [
        pltpu.make_async_copy(source, target, load_sems.at[number])
        for number, (source, target) in enumerate(
            (
                (weight_in, whole_weight.at[slot_rows(hi, inner)]),
                (forget_in, forget_ref),
                (value_in, value_ref),
                (query_in, query_ref),
                (gate_in, gate_ref),
            )
        )
    ]
    for load in loads:
        load.start()

    barrier = pltpu.get_barrier_semaphore()

    peers = members - 1 + tp_size - 1
    for step in range(1, members):
        pl.semaphore_signal(
            barrier,
            inc=1,
            device_id=member_at((member + step) % members),
            device_id_type=MESH_ID,
        )
    for step in range(1, tp_size):
        pl.semaphore_signal(
            barrier, inc=1, device_id={"tp": (tp + step) % tp_size}, device_id_type=MESH_ID
        )
    for step in (1, -1):
        there = line + step
        inside = (there >= 0) & (there < lines)

        @pl.when(inside)
        def _():
            pl.semaphore_signal(barrier, inc=1, device_id=on_line(there), device_id_type=MESH_ID)

        peers = peers + jnp.where(inside, 1, 0)
    pl.semaphore_wait(barrier, peers)

    def piece_lanes(piece):
        return pl.ds(piece * weight_tile, weight_tile)

    def weight_block(block_hi, block_inner, piece):
        return whole_weight.at[slot_rows(block_hi, block_inner), piece_lanes(piece)]

    def step_of(way):
        return 1 if way == 0 else -1

    def line_block(origin, distance, piece):
        block_hi = origin // 2
        if distance % 2 == 0:
            return weight_block(block_hi, inner, piece)
        return relay.at[
            pl.ds(pl.multiple_of(block_hi * depth, depth), depth), piece_lanes(piece)
        ]

    def line_copy(way, hop, piece):
        origin = line - step_of(way) * (hop - 1)
        return remote(
            line_block(origin, hop - 1, piece),
            line_block(origin, hop, piece),
            line_send.at[way, hop - 1],
            line_recv.at[origin, piece],
            on_line(line + step_of(way)),
        )

    def line_arrival(origin, piece):
        block = weight_block(hi, inner, piece)
        return remote(
            block, block, line_send.at[0, 0], line_recv.at[origin, piece], on_line(origin)
        )

    def line_sent(way, hop):
        block = whole_weight.at[slot_rows(hi, inner)]
        return remote(
            block,
            block,
            line_send.at[way, hop - 1],
            line_recv.at[0, 0],
            on_line(line + step_of(way)),
        )

    def inside(index):
        return (index >= 0) & (index < lines)

    def sends(way, hop):
        step = step_of(way)
        last = line + step * (1 + hop % 2)
        return inside(line - step * (hop - 1)) & inside(last)

    def receives(way, hop):
        step = step_of(way)
        return inside(line - step * hop) & inside(line + step * (hop % 2))

    def side_copy(reach, block_hi, piece):
        block = weight_block(block_hi, inner, piece)
        return remote(
            block,
            block,
            side_send.at[reach - 1],
            side_recv.at[reach - 1, block_hi, piece],
            {"inner": (inner + reach) % inner_size},
        )

    def start_line(way, piece):
        @pl.when(sends(way, 1))
        def _():
            line_copy(way, 1, piece).start()

    def start_side(piece):
        for reach in range(1, inner_size):
            side_copy(reach, hi, piece).start()

    def take_hop(hop, way, piece):
        if hop >= lines:
            return
        origin = line - step_of(way) * hop

        @pl.when(receives(way, hop))
        def _():
            line_arrival(origin, piece).wait_recv()
            if hop % 2 == 0:
                for reach in range(1, inner_size):
                    side_copy(reach, origin // 2, piece).start()

        if hop + 1 < lines:

            @pl.when(sends(way, hop + 1))
            def _():
                line_copy(way, hop + 1, piece).start()

    def take_sides(piece):
        for reach in range(1, inner_size):
            for block_hi in range(hi_size):
                side_copy(reach, block_hi, piece).wait_recv()

    def sides_sent():
        for reach in range(1, inner_size):
            remote(
                whole_weight.at[pl.ds(0, hi_size * depth)],
                whole_weight.at[pl.ds(0, hi_size * depth)],
                side_send.at[reach - 1],
                side_recv.at[0, 0, 0],
                {"inner": (inner + reach) % inner_size},
            ).wait_send()

    def state_copy(head):
        return remote(
            state_out.at[head],
            gathered.at[member, head % own_heads],
            gather_send.at[0],
            gather_recv.at[member, head % own_heads],
            member_at(head // own_heads),
        )

    def state_arrival(index, number):
        return remote(
            state_out.at[0],
            gathered.at[index, number],
            gather_send.at[0],
            gather_recv.at[index, number],
            member_at(index),
        )

    def chain_copy(number):
        return remote(
            chain_out.at[number],
            chain_in.at[number],
            chain_send.at[0],
            chain_recv.at[number],
            on_line(line + 1),
        )

    def deliver_copy(index, number):
        head = member * own_heads + number
        return remote(
            deliver_out.at[index * own_heads + number],
            carried.at[head],
            deliver_send.at[0],
            deliver_recv.at[head],
            member_at(index),
        )

    def deliver_arrival(head):
        return remote(
            deliver_out.at[0],
            carried.at[head],
            deliver_send.at[0],
            deliver_recv.at[head],
            member_at(head // own_heads),
        )

    def head_state(head):
        causal = lower_triangle()
        gap = gap_ref[pl.ds(tp * heads + head, 1), :]
        lanes = lanes_of(head)
        this_head = lax.broadcasted_iota(jnp.int32, (heads, SPAN), 0) == head
        state = jnp.zeros((HEAD_DIM, HEAD_DIM), jnp.float32)
        base = jnp.zeros((1, HEAD_DIM), jnp.float32)
        for span in range(spans):
            part = span_rows(span)
            surge = jnp.sum(jnp.where(this_head, surge_ref[:, part], 0.0), axis=0, keepdims=True)
            keys, running = decays(forget_ref[part, lanes], gap, surge, causal)
            keys_ref[part, lanes] = keys
            running_ref[part, lanes] = running
            base_ref[head, span : span + 1, :] = base
            if span > 0:
                starts_ref[head, span - 1] = state.astype(jnp.bfloat16)
            ending = running[SPAN - 1 : SPAN, :]
            kept = (keys * jnp.exp(ending - running)).astype(jnp.bfloat16)
            state = state * jnp.exp(ending) + dot(value_ref[part, lanes], kept, TN)
            base = base + ending
        decay = jnp.exp(base)
        high = decay.astype(jnp.bfloat16).astype(jnp.float32)
        first = lax.broadcasted_iota(jnp.int32, (TAIL, HEAD_DIM), 0) == 0
        item = state.astype(jnp.bfloat16)
        tail = jnp.where(first, high, decay - high).astype(jnp.bfloat16)
        state_out[head, 0:HEAD_DIM, :] = item
        state_out[head, HEAD_DIM:, :] = tail

    def state_body(turn, carry):
        pair = [(turn * 2 + number + (member + 1) * own_heads) % heads for number in range(2)]
        for head in pair:
            head_state(head)
        for head in pair:
            owner = head // own_heads

            @pl.when(owner == member)
            def _():
                gathered[member, head % own_heads] = state_out[head]

            @pl.when(owner != member)
            def _():
                state_copy(head).start()

        return carry

    def chain_states():
        @pl.when(line == 0)
        def _():
            chain_in[...] = jnp.zeros_like(chain_in)

        def body(number, carry):
            for index in range(members):

                @pl.when(member != index)
                def _():
                    state_arrival(index, number).wait_recv()

            @pl.when(line > 0)
            def _():
                chain_copy(number).wait_recv()

            state = chain_in[number].astype(jnp.float32)
            for index in range(members):
                deliver_out[index * own_heads + number] = state.astype(jnp.bfloat16)
                tail = gathered[index, number, HEAD_DIM:, :].astype(jnp.float32)
                item = gathered[index, number, 0:HEAD_DIM, :].astype(jnp.float32)
                state = state * (tail[0:1, :] + tail[1:2, :]) + item
            chain_out[number] = state.astype(jnp.bfloat16)

            @pl.when(line + 1 < lines)
            def _():
                chain_copy(number).start()

            for index in range(members):

                @pl.when(member != index)
                def _():
                    deliver_copy(index, number).start()

            carried[member * own_heads + number] = deliver_out[member * own_heads + number]
            return carry

        lax.fori_loop(0, own_heads, body, 0)

    def take_states():
        def body(head, carry):
            @pl.when(head // own_heads != member)
            def _():
                deliver_arrival(head).wait_recv()

            return carry

        lax.fori_loop(0, heads, body, 0)

    gain = gain_ref[...]

    def local_body(head, carry):
        causal = lower_triangle()
        lanes = lanes_of(head)
        middle = SPAN // 2
        for span in range(spans):
            part = span_rows(span)
            running = running_ref[part, lanes]
            anchor = running[middle - 1 : middle, :]
            queries = silu(query_ref[part, lanes].astype(jnp.float32)) * (HEAD_DIM**-0.5)
            reach = queries * jnp.exp(running - anchor)
            back = keys_ref[part, lanes] * jnp.exp(anchor - running)
            scores = dot(reach.astype(jnp.bfloat16), back.astype(jnp.bfloat16), NT)
            scores = jnp.where(causal, scores, 0.0).astype(jnp.bfloat16)
            out = dot(scores, value_ref[part, lanes])
            if span > 0:
                out = out + dot(
                    (reach * jnp.exp(anchor)).astype(jnp.bfloat16), starts_ref[head, span - 1], NT
                )
            local_ref[part, lanes] = out
            base = base_ref[head, span : span + 1, :]
            reach_ref[part, lanes] = (reach * jnp.exp(anchor + base)).astype(jnp.bfloat16)
            gated_ref[part, lanes] = gain * silu(gate_ref[part, lanes].astype(jnp.float32))
        return carry

    def keeps(index, group):
        return (index * groups + group) % 2 == lo

    def group_lanes(index, group, which):
        start = which * half_width + (index * groups + group) // 2 * per * HEAD_DIM
        return pl.ds(pl.multiple_of(start, HEAD_DIM), per * HEAD_DIM)

    def swap_copy(group, span):
        start = 2 * half_width + group * per * HEAD_DIM
        return remote(
            mixed_ref.at[span_rows(span), pl.ds(start, per * HEAD_DIM)],
            mixed_ref.at[span_rows(span), group_lanes(tp, group, 1)],
            swap_send.at[group // 2],
            swap_recv.at[group // 2, span],
            {"lo": 1 - lo},
        )

    def origin_of(index, mask):
        for bit, by in enumerate(strides):
            if (mask >> bit) & 1:
                index = flipped(index, by)
        return index

    def tp_copy(stage, which, mask, group, span):
        block = mixed_ref.at[span_rows(span), group_lanes(origin_of(tp, mask), group, which)]
        return remote(
            block,
            block,
            tp_send.at[(1 << stage) - 1 + mask, which, group // 2],
            tp_recv.at[(1 << stage) - 1 + mask, which, group // 2, span],
            {"tp": flipped(tp, strides[stage])},
        )

    def mix(span):
        part = span_rows(span)
        for head in range(heads):
            lanes = lanes_of(head)
            out = local_ref[part, lanes] + dot(reach_ref[part, lanes], carried[head], NT)
            mean_sq = jnp.mean(out * out, axis=1, keepdims=True)
            mixed = out * lax.rsqrt(mean_sq + EPSILON) * gated_ref[part, lanes]
            group = head // per
            kept_start = (tp * groups + group) // 2 * per * HEAD_DIM + head % per * HEAD_DIM
            away_start = 2 * half_width + head * HEAD_DIM
            start = jnp.where(keeps(tp, group), kept_start, away_start)
            mixed_ref[part, pl.ds(pl.multiple_of(start, HEAD_DIM), HEAD_DIM)] = mixed.astype(
                jnp.bfloat16
            )

    def send_away(span):
        for group in range(groups):

            @pl.when(jnp.logical_not(keeps(tp, group)))
            def _():
                swap_copy(group, span).start()

    def send_kept(span):
        for group in range(groups):

            @pl.when(keeps(tp, group))
            def _():
                for stage in range(len(strides)):
                    tp_copy(stage, 0, 0, group, span).start()

    def take_swap(span):
        for group in range(groups):

            @pl.when(keeps(tp, group))
            def _():
                swap_copy(group, span).wait_recv()
                for stage in range(len(strides)):
                    tp_copy(stage, 1, 0, group, span).start()

    def take_stage(stage, which, span):
        peer = flipped(tp, strides[stage])
        for mask in range(1 << stage):
            for group in range(groups):

                @pl.when(keeps(origin_of(peer, mask), group))
                def _():
                    tp_copy(stage, which, mask, group, span).wait_recv()
                    for later in range(stage + 1, len(strides)):
                        tp_copy(later, which, mask | (1 << stage), group, span).start()

    def partial_copy(piece, span):
        return remote(
            partial_out.at[piece, span],
            partial_in.at[piece, span],
            partial_send.at[0],
            partial_recv.at[piece, span],
            {"lo": 1 - lo},
        )

    def both(span, start, depth):
        part = span_rows(span)
        return jnp.concatenate(
            [mixed_ref[part, half_width : 2 * half_width], mixed_ref[part, 0:half_width]], axis=0
        )

    def multiply(piece, part):
        lanes = piece_lanes(piece)
        right = whole_weight[:, lanes]
        for span in part:
            total = dot(both(span, 0, half_width), right)
            partial_out[piece, span] = total[0:SPAN].astype(jnp.bfloat16)
            partial_copy(piece, span).start()
            total_ref[span, :, lanes] = total[SPAN:]

    def square_copy(step):
        return remote(
            squares_ref.at[tp],
            squares_ref.at[tp],
            square_send.at[step - 1],
            square_recv.at[step - 1],
            {"tp": (tp + step) % tp_size},
        )

    def combine(piece, span):
        lanes = pl.ds(piece * weight_tile, weight_tile)
        partial_copy(piece, span).wait_recv()
        total = total_ref[span, :, lanes] + partial_in[piece, span].astype(jnp.float32)
        rounded = total.astype(jnp.bfloat16)
        projected_ref[span_rows(span), lanes] = rounded
        branch = rounded.astype(jnp.float32)
        branch = branch * branch
        squares = branch[:, 0:HEAD_DIM]
        for start in range(HEAD_DIM, weight_tile, HEAD_DIM):
            squares = squares + branch[:, start : start + HEAD_DIM]
        if piece > 0:
            squares = squares + sums_ref[span]
        sums_ref[span] = squares

    def total_squares(span):
        column = jnp.sum(sums_ref[span], axis=1, keepdims=True)
        row = jnp.sum(jnp.where(diagonal(), column, 0.0), axis=0, keepdims=True)
        squares_ref[tp, span : span + 1, :] = row

    def finish():
        for step in range(1, tp_size):
            square_copy(step).wait_recv()
        total = squares_ref[0, 0:spans, :]
        for index in range(1, tp_size):
            total = total + squares_ref[index, 0:spans, :]
        scale_ref[...] = lax.rsqrt(total * (1.0 / (columns * tp_size)) + EPSILON)

    def lines_sent(first, last):
        for hop in range(first, last):
            for way in (0, 1):

                @pl.when(sends(way, hop))
                def _():
                    line_sent(way, hop).wait_send()

    def states_sent():
        others = (members - 1) * own_heads
        next_member = member_at((member + 1) % members)
        pltpu.make_async_remote_copy(
            src_ref=state_out.at[pl.ds(0, others)],
            dst_ref=state_out.at[pl.ds(0, others)],
            send_sem=gather_send.at[0],
            recv_sem=gather_recv.at[0, 0],
            device_id=next_member,
            device_id_type=MESH_ID,
        ).wait_send()
        pltpu.make_async_remote_copy(
            src_ref=deliver_out.at[pl.ds(0, others)],
            dst_ref=deliver_out.at[pl.ds(0, others)],
            send_sem=deliver_send.at[0],
            recv_sem=deliver_recv.at[0],
            device_id=next_member,
            device_id_type=MESH_ID,
        ).wait_send()

        @pl.when(line + 1 < lines)
        def _():
            remote(
                chain_out, chain_in, chain_send.at[0], chain_recv.at[0], on_line(line + 1)
            ).wait_send()

    def swaps_sent():
        for group in range(groups):
            block = mixed_ref.at[:, group_lanes(tp, group, 0)]

            @pl.when(jnp.logical_not(keeps(tp, group)))
            def _():
                remote(
                    block, block, swap_send.at[group // 2], swap_recv.at[0, 0], {"lo": 1 - lo}
                ).wait_send()

    def mixed_sent():
        for group in range(groups):
            block = mixed_ref.at[:, group_lanes(tp, group, 0)]

            for stage in range(len(strides)):
                for which in (0, 1):
                    for mask in range(1 << stage):

                        @pl.when(keeps(origin_of(tp, mask), group))
                        def _():
                            remote(
                                block,
                                block,
                                tp_send.at[(1 << stage) - 1 + mask, which, group // 2],
                                tp_recv.at[0, 0, 0, 0],
                                {"tp": flipped(tp, strides[stage])},
                            ).wait_send()

    early = line < 2
    ends = (line == 0) | (line == lines - 1)
    between = jnp.logical_not(ends)
    scope = jax.named_scope

    def local():
        with scope("local"):
            lax.fori_loop(0, heads, local_body, 0)

    def hop_pieces(hop, way, first, last):
        with scope(f"hop{hop}_{way}_{first}"):
            for piece in range(first, last):
                take_hop(hop, way, piece)

    low = line < lines // 2

    def outward(first, last):
        @pl.when(low)
        def _():
            hop_pieces(1, 1, first, last)

        @pl.when(jnp.logical_not(low))
        def _():
            hop_pieces(1, 0, first, last)

    def inward(first, last):
        @pl.when(low)
        def _():
            hop_pieces(1, 0, first, last)

        @pl.when(jnp.logical_not(low))
        def _():
            hop_pieces(1, 1, first, last)

    def own_sides(first, last):
        for piece in range(first, last):
            start_side(piece)

    loads[0].wait()
    for piece in range(pieces):
        if piece < 3:
            start_line(0, piece)
        elif piece == 3:

            @pl.when(line > 0)
            def _():
                start_line(0, piece)

        start_line(1, piece)
    own_sides(0, 1)
    loads[1].wait()
    loads[2].wait()
    with scope("state"):
        lax.fori_loop(0, heads // 2, state_body, 0)
    own_sides(1, 3)
    outward(0, 2)

    @pl.when(jnp.logical_not(low))
    def _():
        hop_pieces(1, 1, 0, 2)

    loads[3].wait()
    loads[4].wait()

    @pl.when(jnp.logical_not(early))
    def _():
        local()

    with scope("chain"):
        chain_states()

    @pl.when(line == 0)
    def _():
        for piece in range(3, 7):
            start_line(0, piece)

    @pl.when(line > 0)
    def _():
        for piece in range(4, pieces):
            start_line(0, piece)

    @pl.when(ends)
    def _():
        own_sides(3, 6)

    @pl.when(between)
    def _():
        own_sides(3, pieces)

    outward(2, 4)

    @pl.when(early)
    def _():
        local()

    def end_hops(first, last):
        @pl.when(ends)
        def _():
            hop_pieces(2, 1, first, last)
            hop_pieces(2, 0, first, last)

    def between_hops(first, last):
        @pl.when(between)
        def _():
            hop_pieces(2, 1, first, last)
            hop_pieces(2, 0, first, last)


    @pl.when(low)
    def _():
        hop_pieces(1, 0, 0, 2)

    inward(2, 4)
    outward(4, 5)
    with scope("take_states"):
        take_states()
    with scope("mix"):
        for span in range(spans):
            mix(span)
            send_away(span)
            if span < 2:
                send_kept(span)


    end_hops(0, 4)
    keeper = keeps(tp, 0)

    @pl.when(jnp.logical_not(keeper))
    def _():
        between_hops(0, 2)

    with scope("swap01"):
        for span in range(2):
            take_swap(span)
            send_kept(span + 2)

    with scope("swapsent"):
        swaps_sent()

    @pl.when(line == 0)
    def _():
        for piece in range(7, pieces):
            start_line(0, piece)

    outward(5, 6)

    @pl.when(jnp.logical_not(low))
    def _():
        hop_pieces(1, 1, 4, pieces)


    @pl.when(keeper)
    def _():
        between_hops(0, 2)


    @pl.when(low)
    def _():
        hop_pieces(1, 0, 4, 6)

    def take_rest(span):
        with scope(f"take{span}"):
            for stage in range(1, len(strides)):
                for which in (0, 1):
                    take_stage(stage, which, span)

    with scope("y0"):
        take_stage(0, 0, 0)
        take_stage(0, 0, 1)
        take_swap(2)
        take_swap(3)
    outward(6, pieces)

    @pl.when(ends)
    def _():
        own_sides(6, pieces)

    if lines <= 4:
        between_hops(2, 4)
    with scope("y1"):
        take_stage(0, 1, 0)
        take_stage(0, 1, 1)
    take_rest(0)
    take_rest(1)
    @pl.when(low)
    def _():
        hop_pieces(1, 0, 6, pieces)

    if lines > 4:
        between_hops(2, pieces)
        end_hops(4, pieces)
    for hop in range(3, lines):
        for way in (0, 1):
            hop_pieces(hop, way, 0, pieces)
    done = []
    order = []

    def advance(part, first, last):
        for piece in range(first, last):
            if not any(piece == other for other, _ in order):
                with scope(f"sides{piece}"):
                    take_sides(piece)
            with scope(f"mult{part[0]}_{piece}"):
                multiply(piece, part)
            order.append((piece, part))
            if len(order) - len(done) > 4:
                settle()

    def settle():
        piece, part = order[len(done)]
        done.append(piece)
        with scope(f"comb{part[0]}_{piece}"):
            for span in part:
                combine(piece, span)

    half_a, half_b = (0, 1), (2, 3)
    advance(half_a, 0, 2)
    with scope("y2"):
        take_stage(0, 0, 2)
        take_stage(0, 0, 3)
    if lines <= 4:
        end_hops(4, 6)
        between_hops(4, 6)
    advance(half_a, 2, 4)
    with scope("y3"):
        take_stage(0, 1, 2)
        take_stage(0, 1, 3)
    take_rest(2)
    take_rest(3)
    if lines <= 4:
        between_hops(6, pieces)
        end_hops(6, pieces)
    advance(half_b, 0, 4)
    states_sent()
    mixed_sent()
    advance(half_a, 4, 6)
    advance(half_b, 4, 6)
    lines_sent(1, lines)
    advance(half_a, 6, pieces)
    advance(half_b, 6, pieces)
    sides_sent()
    while len(order) - len(done) > 1:
        settle()
    with scope("combine_last"):
        settle()
        for span in range(spans):
            total_squares(span)
        for step in range(1, tp_size):
            square_copy(step).start()
    with scope("drain"):
        remote(
            partial_out, partial_in, partial_send.at[0], partial_recv.at[0, 0], {"lo": 1 - lo}
        ).wait_send()
    with scope("finish"):
        finish()
        for step in range(1, tp_size):
            square_copy(step).wait_send()


def layer(sizes, arrays):
    hi_size, inner_size, tp_size, per, tile, weight_tile = sizes
    rows, width = arrays[0].shape
    depth, columns = arrays[7].shape
    heads = width // HEAD_DIM
    groups = heads // per
    spans = rows // SPAN
    members = inner_size
    own_heads = heads // members
    kept = (groups + 1) // 2
    half_width = heads * tp_size // 2 * HEAD_DIM
    pieces = columns // weight_tile
    vmem = pl.BlockSpec(memory_space=pltpu.VMEM)
    anywhere = pl.BlockSpec(memory_space=pl.ANY)
    item = (HEAD_DIM + TAIL, HEAD_DIM)
    square = (HEAD_DIM, HEAD_DIM)
    bf16, f32 = jnp.bfloat16, jnp.float32
    dma = pltpu.SemaphoreType.DMA
    return pl.pallas_call(
        functools.partial(layer_kernel, sizes),
        in_specs=[anywhere] * 4 + [vmem] * 3 + [anywhere],
        out_specs=[vmem, vmem],
        out_shape=[
            pltpu.VMEM((rows, columns), bf16),
            pltpu.VMEM((spans, HEAD_DIM), f32),
        ],
        scratch_shapes=[
            pltpu.VMEM((hi_size * inner_size * depth, columns), bf16),
            pltpu.VMEM((hi_size * depth, columns), bf16),
            pltpu.VMEM((rows, width), bf16),
            pltpu.VMEM((rows, width), bf16),
            pltpu.VMEM((rows, width), bf16),
            pltpu.VMEM((rows, width), bf16),
            pltpu.VMEM((rows, width), f32),
            pltpu.VMEM((rows, width), f32),
            pltpu.VMEM((heads, max(8, spans), HEAD_DIM), f32),
            pltpu.VMEM((heads, max(1, spans - 1)) + square, bf16),
            pltpu.VMEM((heads,) + item, bf16),
            pltpu.VMEM((members, own_heads) + item, bf16),
            pltpu.VMEM((own_heads,) + square, bf16),
            pltpu.VMEM((own_heads,) + square, bf16),
            pltpu.VMEM((heads,) + square, bf16),
            pltpu.VMEM((heads,) + square, bf16),
            pltpu.VMEM((rows, width), f32),
            pltpu.VMEM((rows, width), bf16),
            pltpu.VMEM((rows, width), f32),
            pltpu.VMEM((rows, 2 * half_width + width), bf16),
            pltpu.VMEM((pieces, spans, SPAN, weight_tile), bf16),
            pltpu.VMEM((pieces, spans, SPAN, weight_tile), bf16),
            pltpu.VMEM((spans, SPAN, columns), f32),
            pltpu.VMEM((spans, SPAN, HEAD_DIM), f32),
            pltpu.VMEM((tp_size, max(8, spans), HEAD_DIM), f32),
            dma((5,)),
            dma((1,)),
            dma((members, own_heads)),
            dma((1,)),
            dma((own_heads,)),
            dma((1,)),
            dma((heads,)),
            dma((kept,)),
            dma((kept, spans)),
            dma((tp_size - 1, 2, kept)),
            dma((tp_size - 1, 2, kept, spans)),
            dma((2, 2 * hi_size - 1)),
            dma((2 * hi_size, pieces)),
            dma((inner_size - 1,)),
            dma((inner_size - 1, hi_size, pieces)),
            dma((1,)),
            dma((pieces, spans)),
            dma((tp_size - 1,)),
            dma((tp_size - 1,)),
        ],
        name="layer",
        compiler_params=pltpu.CompilerParams(
            collective_id=0, has_side_effects=True, vmem_limit_bytes=62800 * 1024
        ),
        cost_estimate=pl.CostEstimate(
            flops=rows * width * 10000, bytes_accessed=14 * rows * width, transcendentals=0
        ),
    )(*arrays)


def per_device(hi_size, inner_size, tp_size, *arrays):
    query, forget, value, gate, gap, surge, head_gain, matrix, branch_gain, residual = arrays
    per = inner_size * matrix.shape[0] // HEAD_DIM
    projected, scale = layer(
        (hi_size, inner_size, tp_size, per, 256, 128),
        (
            query,
            forget,
            value,
            gate,
            gap.reshape(-1, HEAD_DIM),
            surge,
            head_gain.reshape(1, HEAD_DIM),
            matrix,
        ),
    )
    columns = matrix.shape[1]
    gain_part = lax.dynamic_slice_in_dim(branch_gain, lax.axis_index("tp") * columns, columns)
    branch = projected.astype(jnp.float32) * scale.reshape(-1)[:, None] * gain_part
    return (residual.astype(jnp.float32) + branch).astype(jnp.bfloat16)


def solution(mesh):
    sp_size, tp_size = mesh.shape["sp"], mesh.shape["tp"]
    sp = ("hi", "lo", "inner")
    placed = (
        P(sp, "tp"),
        P(sp, "tp"),
        P(sp, "tp"),
        P(sp, "tp"),
        P(),
        P("tp", sp),
        P(),
        P(sp, "tp"),
        P(),
        P(sp, "tp"),
    )

    def whole(*arrays):
        inner = max(2, HEAD_DIM * sp_size // arrays[7].shape[0])
        hi = sp_size // (2 * inner)
        devices = mesh.devices.reshape(hi, 2, inner, tp_size)
        paired = Mesh(devices, ("hi", "lo", "inner", "tp"))
        return jax.shard_map(
            functools.partial(per_device, hi, inner, tp_size),
            mesh=paired,
            in_specs=placed,
            out_specs=P(sp, "tp"),
            check_vma=False,
        )(*arrays)

    return whole
```
